128 devices in a mesh: sp: 32 (over z, y, core), tp: 4 (over x).
Axes of the slice: x: 4, y: 4, z: 4, core: 2. Of those that a mesh axis runs over, the one named last changes fastest.
Arguments:
- resid: bfloat16 [16384, 2048], P(('sp', 'tp')), may hold values from -6 to 6
- query: bfloat16 [16384, 2048], P('sp', 'tp'), may hold values from -6 to 6
- forget_logits: bfloat16 [16384, 2048], P('sp', 'tp'), may hold values from -5 to 5
- forget_margin: float32 [2048], P('tp'), may hold values from 0 to 0.07, as said below
- decay_spike: float32 [16384, 16], P('sp', 'tp'), may hold values from -0.75 to 0
- value_logits: bfloat16 [16384, 2048], P('sp', 'tp'), may hold values from -6 to 6
- output_gate_logits: bfloat16 [16384, 2048], P('sp', 'tp'), may hold values from -6 to 6
- head_norm_scale: float32 [2048], P('tp'), may hold values from 0.1 to 1.9
- output_matrix: bfloat16 [2048, 2048], replicated, may hold values from -0.125 to 0.125
- norm_scale_vector: float32 [2048], replicated, may hold values from 0.1 to 1.9
- routes: int32 [16384, 2], P(('sp', 'tp')), may hold values from 0 to 127, all different within a row; in each aligned block of 128 rows (0 to 127, 128 to 255, ...) at most 4 rows name the same one
- routing_weight: float32 [16384, 2], P(('sp', 'tp')), may hold values from 0.2 to 1
- gate_matrix: bfloat16 [128, 2048, 1024], P(('sp', 'tp')), may hold values from -0.125 to 0.125
- up_matrix: bfloat16 [128, 2048, 1024], P(('sp', 'tp')), may hold values from -0.125 to 0.125
- down_matrix: bfloat16 [128, 1024, 2048], P(('sp', 'tp')), may hold values from -0.1875 to 0.1875
Outputs:
- result: bfloat16 [16384, 2048], P(('sp', 'tp'))
The draws below stay inside these ranges and needn't reach their ends.
Inputs may be any that keep to these rules, and one draw needn't show every extreme that they name: `routes`: within the rows of one device no expert is named by more than 4 rows; some device names some expert exactly 4 times in every draw. `forget_margin`: Positive.
All inputs are finite; a program needn't handle non-finite values.
Results may differ from the reference program's by a relative error of at most 0.012.
Values may be sent and summed in bfloat16 or wider, within the bound.
No kernel may reach another device: no remote copies, remote signals or barrier semaphores. Data moves between devices by JAX's collectives and lax.ppermute only.
A program may use at most 128 MiB of HBM per device.

```python
import math
import jax
import jax.numpy as jnp
import numpy as np
from jax import lax

D = 2048
HEAD_TOTAL = 16
DK = 128
DV = 128
FF = 1024
TOP = 2
BLOCK = 64
TOKENS_PER_SHARD = 512
SEQUENCE_TOKENS = 16384
ROWS = 128
EXPERTS = 128
CAP = 4
DEVICES = 128


def slow_choice(key):
    pick_key, slow_key, fast_key = jax.random.split(jax.random.fold_in(key, 11), 3)
    ranking = jax.random.permutation(pick_key, HEAD_TOTAL)
    slow_heads = ranking < HEAD_TOTAL // 2
    return (slow_heads, slow_key, fast_key)


def draw_forget_margin(key, part):
    slow_heads, slow_key, fast_key = slow_choice(key)
    slow_gap = jnp.exp(jax.random.uniform(slow_key, (HEAD_TOTAL, DK), jnp.float32, jnp.log(0.3), jnp.log(1.5))) / SEQUENCE_TOKENS
    fast_gap = jnp.exp(jax.random.uniform(fast_key, (HEAD_TOTAL, DK), jnp.float32, jnp.log(0.02), jnp.log(0.066)))
    return jnp.where(slow_heads[:, None], slow_gap, fast_gap).reshape(HEAD_TOTAL * DK)


def draw_forget_logits(key, part):
    jitter_key, shift_key = jax.random.split(jax.random.fold_in(key, 23))
    block_count = SEQUENCE_TOKENS // TOKENS_PER_SHARD
    shifts = jax.random.uniform(shift_key, (block_count, HEAD_TOTAL), jnp.float32, -1.0, 1.0)
    jitter = jnp.clip(jax.random.normal(jitter_key, (SEQUENCE_TOKENS, HEAD_TOTAL * DK), jnp.float32), -4.0, 4.0)
    block_shift = jnp.repeat(jnp.repeat(shifts, TOKENS_PER_SHARD, axis=0), DK, axis=1)
    return (jitter + block_shift).astype(jnp.bfloat16)


def draw_decay_spike(key, part):
    slow_heads, slow_key, fast_key = slow_choice(key)
    position_seed, spike_size_seed, rate_seed = jax.random.split(jax.random.fold_in(key, 37), 3)
    spike_positions = jax.random.randint(position_seed, (3, HEAD_TOTAL), 0, SEQUENCE_TOKENS)
    spike_magnitudes = jnp.log(jax.random.uniform(spike_size_seed, (3, HEAD_TOTAL), jnp.float32, 0.5, 0.8))
    position_entries = jnp.arange(SEQUENCE_TOKENS, dtype=jnp.int32)[:, None, None] == spike_positions[None, :, :]
    spike_events = jnp.sum(jnp.where(position_entries, spike_magnitudes[None, :, :], 0.0), axis=1)
    block_count = SEQUENCE_TOKENS // TOKENS_PER_SHARD
    additional_rate = -jax.random.uniform(rate_seed, (block_count, HEAD_TOTAL), jnp.float32, 0.005, 0.045)
    additional_rate = jnp.where(slow_heads[None, :], 0.0, additional_rate)
    return spike_events + jnp.repeat(additional_rate, TOKENS_PER_SHARD, axis=0)


def shard_levels(own_key, extent, pieces, low, top_value):
    gain = 1.0
    for axis_at, blocks in pieces:
        draws = jax.random.uniform(jax.random.fold_in(jax.random.fold_in(own_key, 6), axis_at), (blocks,), jnp.float32, low / len(pieces), top_value / len(pieces))
        gain = gain * jnp.repeat(jnp.exp(draws), extent[axis_at] // blocks).reshape((-1,) + (1,) * (len(extent) - 1 - axis_at))
    return gain


def shared_out(stream_key, own, number, rows, amount, top, reach, slope):
    order = jax.random.permutation(stream_key, amount)
    heavy_load, common = load_shares(amount, rows * top, reach, slope, True), load_shares(amount, rows * top, reach, slope, False)
    places = jnp.arange(amount)

    def named(sizes, offset_by):
        used = int((sizes > 0).sum())
        fixed = max(1, used // 4)
        passed = fixed + (places - fixed + offset_by * (used - fixed)) % max(1, amount - fixed)
        return jnp.zeros((amount,), jnp.int32).at[order[jnp.where(places < fixed, places, passed)]].set(jnp.asarray(sizes, jnp.int32))

    sizes = jnp.where(number % 4 == 0, named(heavy_load, number // 4), named(common, number - number // 4 - 1))
    mixed = jax.random.permutation(jax.random.fold_in(own, 3), amount)
    giver, taker = mixed[0:amount // 2 * 2:2], mixed[1:amount // 2 * 2:2]
    slack = jnp.minimum(sizes[giver] - 1, reach - sizes[taker]) // 2
    slack = jnp.where((giver == order[0]) | (taker == order[0]) | (sizes[taker] == 0), 0, jnp.maximum(slack, 0))
    passed = jax.random.randint(jax.random.fold_in(own, 4), (amount // 2,), 0, 1 << 20) % (slack + 1)
    sizes = sizes.at[giver].add(-passed).at[taker].add(passed)
    members = jnp.searchsorted(jnp.cumsum(sizes), jnp.arange(rows * top), side="right").astype(jnp.int32)
    grid = members.reshape(top, rows).T
    grid = grid[jax.random.permutation(jax.random.fold_in(own, 1), rows)]
    offset_by = jax.random.randint(jax.random.fold_in(own, 2), (rows, 1), 0, top)
    return jnp.take_along_axis(grid, (jnp.arange(top)[None, :] + offset_by) % top, axis=1)


def load_shares(amount, total, limit, slope, full):
    loads = [(1 << 20) // math.isqrt(standing ** slope) + 1 for standing in range(1, amount + 1)]
    largest = limit if full else min(limit, max(-(-total // amount), total * loads[0] // sum(loads)))
    least = 1 if total - largest >= amount - 1 else 0
    holding, spare = [largest] + [least] * (amount - 1), total - largest - least * (amount - 1)
    while spare > 0:
        movable = [i for i in range(1, amount) if holding[i] < largest] or [i for i in range(1, amount) if holding[i] < limit]
        whole, left = sum([loads[i] for i in movable]), spare
        for i in movable:
            extra = min(limit - holding[i], max(1, left * loads[i] // whole), spare)
            holding[i] = holding[i] + extra
            spare = spare - extra
    return np.array(holding)


def centred(key, dims, deviation, most, pieces=(), held_as=jnp.bfloat16):
    drawn = jax.random.normal(key, dims, jnp.float32) * deviation
    if len(pieces) > 0:
        drawn = shard_levels(key, dims, pieces, -0.22, 0.18) * drawn
    return jnp.clip(drawn, min=-most, max=most).astype(held_as)


def setup_inputs(seed: int = 0) -> dict:
    splits = jax.random.split(jax.random.key(seed), 16)
    resid = centred(splits[0], (SEQUENCE_TOKENS, D), 1.0, 6.0, ((0, 128),))
    query = centred(splits[1], (SEQUENCE_TOKENS, HEAD_TOTAL * DK), 1.0, 6.0, ((0, 32), (1, 4)))
    forget_logits = draw_forget_logits(jax.random.fold_in(splits[15], 71), 0)
    forget_margin = draw_forget_margin(jax.random.fold_in(splits[15], 71), 0)
    decay_spike = draw_decay_spike(jax.random.fold_in(splits[15], 71), 0)
    value_logits = centred(splits[5], (SEQUENCE_TOKENS, HEAD_TOTAL * DV), 1.0, 6.0, ((0, 32), (1, 4)))
    output_gate_logits = centred(splits[6], (SEQUENCE_TOKENS, HEAD_TOTAL * DV), 1.0, 6.0, ((0, 32), (1, 4)))
    head_norm_scale = jnp.clip(1.0 + 0.18 * jax.random.normal(splits[7], (HEAD_TOTAL * DV,), jnp.float32), 0.1, 1.9)
    output_matrix = centred(splits[8], (HEAD_TOTAL * DV, D), (HEAD_TOTAL * DV) ** -0.5, 0.125)
    norm_scale_vector = jnp.clip(1.0 + 0.18 * jax.random.normal(splits[9], (D,), jnp.float32), 0.1, 1.9)
    routes_keys = jax.random.split(jax.random.fold_in(splits[10], 1), SEQUENCE_TOKENS // ROWS)
    routes_turns = jax.random.permutation(jax.random.fold_in(splits[10], 3), SEQUENCE_TOKENS // ROWS)
    routes = jax.vmap(lambda own, number: shared_out(jax.random.fold_in(splits[10], 2), own, number, ROWS, EXPERTS, TOP, CAP, 2))(routes_keys, routes_turns).reshape((SEQUENCE_TOKENS, TOP))
    routing_weight = jnp.clip(0.2 + 0.8 * jax.random.uniform(splits[11], (SEQUENCE_TOKENS, TOP), jnp.float32) ** shard_levels(splits[11], (SEQUENCE_TOKENS, TOP), ((0, 128),), -0.2, 0.2), 0.2, 1.0)
    gate_matrix = centred(splits[12], (EXPERTS, D, FF), D ** -0.5, 0.125, ((0, 128),))
    up_matrix = centred(splits[13], (EXPERTS, D, FF), D ** -0.5, 0.125, ((0, 128),))
    down_matrix = centred(splits[14], (EXPERTS, FF, D), FF ** -0.5, 0.1875, ((0, 128),))
    return {"resid": resid, "query": query, "forget_logits": forget_logits, "forget_margin": forget_margin, "decay_spike": decay_spike, "value_logits": value_logits, "output_gate_logits": output_gate_logits, "head_norm_scale": head_norm_scale, "output_matrix": output_matrix, "norm_scale_vector": norm_scale_vector, "routes": routes, "routing_weight": routing_weight, "gate_matrix": gate_matrix, "up_matrix": up_matrix, "down_matrix": down_matrix}


maximum_value = lax.Precision.HIGHEST

def to_blocks(matrix, head_number):
    length, columns = matrix.shape
    return matrix.reshape(length // BLOCK, BLOCK, head_number, columns // head_number).transpose(0, 2, 1, 3)

def from_blocks(matrix):
    block_count, head_number, span_len, head_width = matrix.shape
    return matrix.transpose(0, 2, 1, 3).reshape(block_count * span_len, head_number * head_width)

def input_lookup(query, forget_logits, forget_margin, decay_spike, value_logits):
    head_number = decay_spike.shape[1]
    every_key = forget_margin[None, :] * jax.nn.sigmoid(-forget_logits.astype(jnp.float32))
    head_width = every_key.shape[1] // head_number
    logarithm_of_decay = jnp.log1p(-every_key) + jnp.repeat(decay_spike, head_width, axis=1)
    queries = query.astype(jnp.float32) * DK ** (-0.5)
    values = jax.nn.silu(value_logits.astype(jnp.float32))
    return (to_blocks(queries, head_number), to_blocks(every_key, head_number), to_blocks(values, head_number), to_blocks(logarithm_of_decay, head_number))

def block_recurrence(queries, keys_in, values, logarithm_of_decay):
    span_len = queries.shape[2]
    causal = (lax.broadcasted_iota(jnp.int32, (span_len, span_len), 0) >= lax.broadcasted_iota(jnp.int32, (span_len, span_len), 1))[:, :, None]
    cum_log = jnp.cumsum(logarithm_of_decay, axis=2)

    def advance(current_state, inputs):
        query_block, key_b, value_block, cumulative_block = inputs
        spread = cumulative_block[:, :, None, :] - cumulative_block[:, None, :, :]
        weight_t = jnp.where(causal, jnp.exp(jnp.where(causal, spread, 0.0)), 0.0)
        router_scores = jnp.einsum('htk,hsk,htsk->hts', query_block, key_b, weight_t, precision=maximum_value)
        within = jnp.einsum('hts,hsv->htv', router_scores, value_block, precision=maximum_value)
        incoming_state = jnp.einsum('bup,bpl->bul', query_block * jnp.exp(cumulative_block), current_state, precision=maximum_value)
        final_block = cumulative_block[:, -1, :]
        decayed_state = key_b * jnp.exp(final_block[:, None, :] - cumulative_block)
        following_state = jnp.exp(final_block)[:, :, None] * current_state + jnp.einsum('ixq,ixn->iqn', decayed_state, value_block, precision=maximum_value)
        return (following_state, within + incoming_state)
    start_state = jnp.zeros((queries.shape[1], queries.shape[3], values.shape[3]), jnp.float32)
    last_state, outputs = lax.scan(advance, start_state, (queries, keys_in, values, cum_log))
    return (last_state, outputs, cum_log)

def gate_rows(recurrence_output, output_gate_logits, head_norm_scale):
    square = lax.optimization_barrier(jnp.mean(recurrence_output * recurrence_output, axis=3, keepdims=True))
    scaled = from_blocks(recurrence_output * lax.rsqrt(square + 1e-06)) * head_norm_scale[None, :]
    return (scaled * jax.nn.silu(output_gate_logits.astype(jnp.float32))).astype(jnp.bfloat16)

def row_norm(stream, norm_scale_vector):
    values = stream.astype(jnp.float32)
    square = lax.optimization_barrier(jnp.mean(values * values, axis=1, keepdims=True))
    return (values * lax.rsqrt(square + 1e-06) * norm_scale_vector[None, :]).astype(jnp.bfloat16)

def reference(resid, query, forget_logits, forget_margin, decay_spike, value_logits, output_gate_logits, head_norm_scale, output_matrix, norm_scale_vector, routes, routing_weight, gate_matrix, up_matrix, down_matrix):
    block_list = input_lookup(query, forget_logits, forget_margin, decay_spike, value_logits)
    last_state, recurrence_output, cum_log = block_recurrence(*block_list)
    gated_rows = gate_rows(recurrence_output, output_gate_logits, head_norm_scale)
    mixed_rows = jnp.dot(gated_rows, output_matrix, preferred_element_type=jnp.float32)
    stream = (resid.astype(jnp.float32) + mixed_rows).astype(jnp.bfloat16)
    normed = row_norm(stream, norm_scale_vector)
    flat_routes = routes.reshape(-1)
    member = (flat_routes[:, None] == jnp.arange(EXPERTS, dtype=jnp.int32)[None, :]).astype(jnp.int32)
    slot_rank = lax.optimization_barrier(jnp.sum(jnp.cumsum(member, axis=0) * member, axis=1)) - 1
    slot_depth = DEVICES * CAP
    position_entries = (flat_routes * slot_depth + slot_rank).astype(jnp.int32)
    sources = (jnp.arange(flat_routes.shape[0], dtype=jnp.int32) // TOP).astype(jnp.int32)
    buffer = jnp.zeros((EXPERTS * slot_depth, D), jnp.bfloat16).at[position_entries].set(normed[sources])

    def expert_rows(inputs):
        slot_rows, gate_e, up_e, down_e = inputs
        gate_part = jnp.dot(slot_rows, gate_e, preferred_element_type=jnp.float32)
        up_part = jnp.dot(slot_rows, up_e, preferred_element_type=jnp.float32)
        hidden = (jax.nn.silu(gate_part) * up_part).astype(jnp.bfloat16)
        return jnp.dot(hidden, down_e, preferred_element_type=jnp.float32).astype(jnp.bfloat16)
    outputs = lax.map(expert_rows, (buffer.reshape(EXPERTS, slot_depth, D), gate_matrix, up_matrix, down_matrix))
    picked = outputs.reshape(EXPERTS * slot_depth, D)[position_entries].astype(jnp.float32).reshape(-1, TOP, D)
    combined = stream.astype(jnp.float32) + lax.optimization_barrier(jnp.sum(routing_weight[:, :, None] * picked, axis=1))
    return combined.astype(jnp.bfloat16)
```

```python
import functools

import jax
import jax.numpy as jnp
from jax import lax
from jax.experimental import pallas as pl
from jax.experimental.pallas import tpu as pltpu
from jax.sharding import Mesh
from jax.sharding import PartitionSpec as P

DK = 128
CHUNK = 128
SP = ("sp_0", "sp_1", "sp_2")
SP_TP = ("sp_0", "sp_1", "sp_2", "tp")
F32 = jnp.float32
BF16 = jnp.bfloat16


def dot_nn(a, b):
    return lax.dot_general(a, b, (((1,), (0,)), ((), ())), preferred_element_type=F32)


def dot_nt(a, b):
    return lax.dot_general(a, b, (((1,), (1,)), ((), ())), preferred_element_type=F32)


def dot_tn(a, b):
    return lax.dot_general(a, b, (((0,), (0,)), ((), ())), preferred_element_type=F32)


def lower_mask(n, strict):
    row = lax.broadcasted_iota(jnp.int32, (n, n), 0)
    col = lax.broadcasted_iota(jnp.int32, (n, n), 1)
    return row > col if strict else row >= col


def in_hbm(value):
    return pltpu.with_memory_space_constraint(value, pltpu.HBM)


def params(mebibytes):
    return pltpu.CompilerParams(vmem_limit_bytes=mebibytes * 1024 * 1024)


def halves(value):
    high = value.astype(BF16)
    return high, (value - high.astype(F32)).astype(BF16)


def state_kernel(forget_ref, value_ref, margin_ref, spike_ref, cum_ref, values_ref, start_ref, sent_ref, state, before):
    step = pl.program_id(0)
    heads = forget_ref.shape[1] // DK

    @pl.when(step == 0)
    def _():
        state[...] = jnp.zeros_like(state)
        before[...] = jnp.zeros_like(before)

    tri = lower_mask(CHUNK, False).astype(BF16)
    for c in range(forget_ref.shape[0] // CHUNK):
        rows = slice(c * CHUNK, (c + 1) * CHUNK)
        spikes = halves(spike_ref[:, rows])
        spikes = dot_nt(tri, spikes[0]) + dot_nt(tri, spikes[1])
        start_ref[c] = state[...]
        for h in range(heads):
            cols = slice(h * DK, (h + 1) * DK)
            keys = margin_ref[:, cols] / (1.0 + jnp.exp(forget_ref[rows, cols].astype(F32)))
            high, low = halves(jnp.log(1.0 - keys))
            cum = dot_nn(tri, high) + dot_nn(tri, low) + spikes[:, h : h + 1]
            cum_ref[rows, cols] = cum
            last = cum[CHUNK - 1 : CHUNK, :]
            logits = value_ref[rows, cols].astype(F32)
            values = (logits / (1.0 + jnp.exp(-logits))).astype(BF16)
            values_ref[rows, cols] = values
            kept = (keys * jnp.exp(last - cum)).astype(BF16)
            state[cols, :] = jnp.exp(last) * state[cols, :] + dot_tn(values, kept)
            before[:, cols] = before[:, cols] + last

    @pl.when(step == pl.num_programs(0) - 1)
    def _():
        share = DK // 8
        first = lax.broadcasted_iota(jnp.int32, (share, DK), 0) == 0
        for h in range(heads):
            total = before[:, h * DK : (h + 1) * DK]
            high = total.astype(BF16).astype(F32)
            tail = jnp.where(first, high, total - high).astype(BF16)
            for i in range(8):
                row = h * DK + i * share
                sent_ref[h * 8 + i, 0:share, :] = state[row : row + share, :].astype(BF16)
                sent_ref[h * 8 + i, share : 2 * share, :] = tail


STATE_STEPS = 2


def local_states(forget_logits, value_logits, margin, spike):
    rows, width = forget_logits.shape
    heads = width // DK
    size = rows // STATE_STEPS
    by_rows = lambda i: (i, 0)
    return pl.pallas_call(
        state_kernel,
        grid=(STATE_STEPS,),
        in_specs=[
            pl.BlockSpec((size, width), by_rows),
            pl.BlockSpec((size, width), by_rows),
            pl.BlockSpec((1, width), lambda i: (0, 0)),
            pl.BlockSpec((heads, size), lambda i: (0, i)),
        ],
        out_specs=[
            pl.BlockSpec((size, width), by_rows),
            pl.BlockSpec((size, width), by_rows),
            pl.BlockSpec((size // CHUNK, width, DK), lambda i: (i, 0, 0)),
            pl.BlockSpec((heads * 8, 2 * DK // 8, DK), lambda i: (0, 0, 0)),
        ],
        out_shape=[
            pltpu.HBM((rows, width), F32),
            pltpu.HBM((rows, width), BF16),
            pltpu.HBM((rows // CHUNK, width, DK), F32),
            pltpu.HBM((heads * 8, 2 * DK // 8, DK), BF16),
        ],
        scratch_shapes=[pltpu.VMEM((width, DK), F32), pltpu.VMEM((1, width), F32)],
        compiler_params=params(16),
        name="local_states",
    )(*map(in_hbm, (forget_logits, value_logits, margin, spike)))


def carry_kernel(parts_ref, prior_ref):
    share = prior_ref.shape[1]
    running = jnp.zeros(prior_ref.shape[1:], F32)
    for d in range(parts_ref.shape[0]):
        prior_ref[d] = running
        tail = parts_ref[d, share : 2 * share, :].astype(F32)
        total = tail[0:1, :] + tail[1:2, :]
        running = jnp.exp(total) * running + parts_ref[d, 0:share, :].astype(F32)


def carried_in(parts):
    return pl.pallas_call(
        carry_kernel,
        out_shape=jax.ShapeDtypeStruct((parts.shape[0], parts.shape[1] // 2, parts.shape[2]), F32),
        compiler_params=params(8),
        name="carried_in",
    )(parts)


def dot_split(queries, states):
    return dot_nt(queries[0], states[0]) + dot_nt(queries[0], states[1]) + dot_nt(queries[1], states[0])


def within_kernel(query_ref, forget_ref, margin_ref, cum_ref, values_ref, start_ref, gate_ref, scale_ref, out_ref, high_ref, low_ref, gates_ref, before):
    heads = query_ref.shape[1] // DK
    causal = lower_mask(CHUNK, False)

    @pl.when(pl.program_id(0) == 0)
    def _():
        before[...] = jnp.zeros_like(before)

    for h in range(heads):
        cols = slice(h * DK, (h + 1) * DK)
        cum = cum_ref[:, cols]
        spread = cum - cum[CHUNK // 2 - 1 : CHUNK // 2, :]
        keys = margin_ref[:, cols] / (1.0 + jnp.exp(forget_ref[:, cols].astype(F32)))
        queries = query_ref[:, cols].astype(F32) * (DK**-0.5)
        scores = dot_nt((queries * jnp.exp(spread)).astype(BF16), (keys * jnp.exp(-spread)).astype(BF16))
        scores = jnp.where(causal, scores, 0.0).astype(BF16)
        decayed = queries * jnp.exp(cum)
        earlier = dot_split(halves(decayed), halves(start_ref[0, cols, :]))
        out_ref[:, cols] = dot_nn(scores, values_ref[:, cols]) + earlier
        high_ref[:, cols], low_ref[:, cols] = halves(decayed * jnp.exp(before[:, cols]))
        before[:, cols] = before[:, cols] + cum[CHUNK - 1 : CHUNK, :]
        logits = gate_ref[:, cols].astype(F32)
        gates_ref[:, cols] = scale_ref[:, cols] * (logits / (1.0 + jnp.exp(-logits)))


def within_blocks(query, forget_logits, margin, cum, values, start, gate_logits, scale):
    rows, width = query.shape
    block = pl.BlockSpec((CHUNK, width), lambda i: (i, 0))
    row = pl.BlockSpec((1, width), lambda i: (0, 0))
    return pl.pallas_call(
        within_kernel,
        grid=(rows // CHUNK,),
        in_specs=[block, block, row, block, block, pl.BlockSpec((1, width, DK), lambda i: (i, 0, 0)), block, row],
        out_specs=[block, block, block, block],
        out_shape=[pltpu.HBM((rows, width), kind) for kind in (F32, BF16, BF16, F32)],
        scratch_shapes=[pltpu.VMEM((1, width), F32)],
        compiler_params=params(16),
        name="within_blocks",
    )(*map(in_hbm, (query, forget_logits, margin, cum, values, start, gate_logits, scale)))


def readout_kernel(place_ref, within_ref, high_ref, low_ref, prior_ref, gates_ref, *out_refs):
    step = pl.program_id(0)
    heads = within_ref.shape[1] // DK
    parts = []
    for h in range(heads):
        cols = slice(h * DK, (h + 1) * DK)
        carried = dot_split((high_ref[:, cols], low_ref[:, cols]), halves(prior_ref[cols, :]))
        recurrent = within_ref[:, cols] + carried
        square = jnp.mean(recurrent * recurrent, axis=1, keepdims=True)
        parts.append((recurrent * lax.rsqrt(square + 1e-06) * gates_ref[:, cols]).astype(BF16))
    for k, out_ref in enumerate(out_refs):

        @pl.when(step == k)
        def _():
            for h in range(heads):
                out_ref[:, h * DK : (h + 1) * DK] = parts[h]


def gated_rows(place, within, high, low, prior, gates):
    rows, width = within.shape
    steps = rows // CHUNK
    block = pl.BlockSpec((CHUNK, width), lambda i, place: ((place[0] + i) % steps, 0))
    return pl.pallas_call(
        readout_kernel,
        grid_spec=pltpu.PrefetchScalarGridSpec(
            num_scalar_prefetch=1,
            grid=(steps,),
            in_specs=[block, block, block, pl.BlockSpec((width, DK), lambda i, place: (0, 0)), block],
            out_specs=[pl.BlockSpec((CHUNK, width), lambda i, place: (0, 0))] * steps,
        ),
        out_shape=[jax.ShapeDtypeStruct((CHUNK, width), BF16)] * steps,
        compiler_params=params(16),
        name="gated_rows",
    )(place, in_hbm(within), in_hbm(high), in_hbm(low), prior, in_hbm(gates))


def slot_positions(routes, experts, capacity):
    rows = routes.shape[0]
    lanes = lax.broadcasted_iota(jnp.int32, (rows, experts), 1)
    first, second = (routes[:, 0:1], routes[:, 1:2])
    one, two = (lanes == first, lanes == second)
    named = (one.astype(F32) + two.astype(F32)).astype(BF16)
    earlier = dot_nn(lower_mask(rows, True).astype(BF16), named)
    ranks = [
        jnp.sum(jnp.where(hit, earlier, 0.0), axis=1, keepdims=True).astype(jnp.int32)
        for hit in (one, two)
    ]
    return [expert * (2 * capacity) + rank for expert, rank in zip((first, second), ranks)]


def own_kernel(place_ref, own_ref, matrix_ref, resid_ref, routes_ref, total_ref, select_ref, pick_ref, *, experts, capacity):
    total_ref[...] = resid_ref[...].astype(F32) + dot_nn(own_ref[...], matrix_ref[...])
    rows = routes_ref.shape[0]
    slots = 2 * experts * capacity
    places = slot_positions(routes_ref[...], experts, capacity)
    lanes = lax.broadcasted_iota(jnp.int32, (rows, slots), 1)
    down = lax.broadcasted_iota(jnp.int32, (slots, rows), 0)
    across = [
        jnp.transpose(jnp.broadcast_to(place.astype(F32), (rows, rows)))[0:1, :].astype(jnp.int32)
        for place in places
    ]
    for j in range(2):
        hit = (down == across[0] + j * capacity) | (down == across[1] + j * capacity)
        select_ref[:, j * rows : (j + 1) * rows] = jnp.where(hit, 1.0, 0.0).astype(BF16)
        for k in range(2):
            at = (2 * j + k) * rows
            pick_ref[at : at + rows, :] = jnp.where(lanes == places[k] + j * capacity, 1.0, 0.0).astype(BF16)


def project_own(place, own, matrix, resid, routes, experts, capacity):
    rows, inner = own.shape
    width = matrix.shape[1]
    slots = 2 * experts * capacity
    fixed = lambda i, place: (0, 0)
    return pl.pallas_call(
        functools.partial(own_kernel, experts=experts, capacity=capacity),
        grid_spec=pltpu.PrefetchScalarGridSpec(
            num_scalar_prefetch=1,
            grid=(1,),
            in_specs=[
                pl.BlockSpec((rows, inner), fixed),
                pl.BlockSpec((inner, width), lambda i, place: (place[0], 0)),
                pl.BlockSpec((rows, width), fixed),
                pl.BlockSpec(routes.shape, fixed),
            ],
            out_specs=[
                pl.BlockSpec((rows, width), fixed),
                pl.BlockSpec((slots, 2 * rows), fixed),
                pl.BlockSpec((4 * rows, slots), fixed),
            ],
        ),
        out_shape=[
            jax.ShapeDtypeStruct((rows, width), F32),
            jax.ShapeDtypeStruct((slots, 2 * rows), BF16),
            jax.ShapeDtypeStruct((4 * rows, slots), BF16),
        ],
        compiler_params=params(24),
        name="project_own",
    )(place, own, in_hbm(matrix), in_hbm(resid), routes)


def project_kernel(place_ref, first_ref, second_ref, third_ref, matrix_ref, own_ref, scale_ref, select_ref, stream_ref, packed_ref, total, stacked):
    step = pl.program_id(0)
    for k, part_ref in enumerate((first_ref, second_ref, third_ref)):

        @pl.when(step == k)
        def _():
            total[...] = (own_ref if k == 0 else total)[...] + dot_nn(part_ref[...], matrix_ref[...])

    @pl.when(step == 2)
    def _():
        stream = total[...].astype(BF16)
        stream_ref[...] = stream
        values = stream.astype(F32)
        square = jnp.mean(values * values, axis=1, keepdims=True)
        normed = (values * lax.rsqrt(square + 1e-06) * scale_ref[...]).astype(BF16)
        rows, width = normed.shape
        half = width // 2
        stacked[0:rows, :] = normed[:, :half]
        stacked[rows : 2 * rows, :] = normed[:, half:]

    wide = packed_ref.shape[1]
    for n in range(stacked.shape[1] // wide):

        @pl.when(step == n + 2)
        def _():
            packed_ref[...] = dot_nn(select_ref[...], stacked[:, n * wide : (n + 1) * wide]).astype(BF16)


def project(place, arrived, shifts, matrix, own_total, scale, select):
    rows, inner = arrived[0].shape
    width = matrix.shape[1]
    parts = matrix.shape[0] // inner
    slots = select.shape[0]
    split = 4
    fixed = lambda i, place: (0, 0)

    def source(i, place):
        shift = jnp.where(i == 0, shifts[0], jnp.where(i == 1, shifts[1], shifts[2]))
        return ((place[0] + parts - shift) % parts, 0)

    return pl.pallas_call(
        project_kernel,
        grid_spec=pltpu.PrefetchScalarGridSpec(
            num_scalar_prefetch=1,
            grid=(2 + split,),
            in_specs=[
                pl.BlockSpec((rows, inner), fixed),
                pl.BlockSpec((rows, inner), fixed),
                pl.BlockSpec((rows, inner), fixed),
                pl.BlockSpec((inner, width), source),
                pl.BlockSpec((rows, width), fixed),
                pl.BlockSpec((1, width), fixed),
                pl.BlockSpec(select.shape, fixed),
            ],
            out_specs=[
                pl.BlockSpec((rows, width), fixed),
                pl.BlockSpec((slots, width // 2 // split), lambda i, place: (0, jnp.maximum(i - 2, 0))),
            ],
            scratch_shapes=[pltpu.VMEM((rows, width), F32), pltpu.VMEM((2 * rows, width // 2), BF16)],
        ),
        out_shape=[
            pltpu.HBM((rows, width), BF16),
            jax.ShapeDtypeStruct((slots, width // 2), BF16),
        ],
        compiler_params=params(24),
        name="project",
    )(place, *arrived, in_hbm(matrix), own_total, in_hbm(scale), select)


def expert_kernel(slots_ref, gate_ref, up_ref, down_ref, out_ref, rows_in, hidden, gate_in, up_in, down_in, outs, sems):
    half = slots_ref.shape[1]
    split, wide = (gate_in.shape[0], gate_in.shape[2])
    cols = [slice(i * wide, (i + 1) * wide) for i in range(split)]
    gate_copies = [pltpu.make_async_copy(gate_ref.at[0, :, cols[i]], gate_in.at[i], sems.at[0, i]) for i in range(split)]
    up_copies = [pltpu.make_async_copy(up_ref.at[0, :, cols[i]], up_in.at[i], sems.at[1, i]) for i in range(split)]
    down_copies = [
        [
            pltpu.make_async_copy(
                down_ref.at[0, :, j * half + i * wide : j * half + (i + 1) * wide], down_in.at[i, j], sems.at[2 + j, i]
            )
            for j in range(2)
        ]
        for i in range(split)
    ]
    out_copies = [pltpu.make_async_copy(outs.at[i], out_ref.at[:, cols[i]], sems.at[4, i]) for i in range(split)]
    for i in range(split):
        gate_copies[i].start()
        up_copies[i].start()
    for i in range(split):
        down_copies[i][0].start()
        down_copies[i][1].start()

    group = 64
    upper = lax.broadcasted_iota(jnp.int32, (group // 16, 8, half), 1) < 4

    def untangle(i, carry):
        block = slots_ref[pl.ds(i * group, group), :].astype(F32).reshape(group // 16, 2, 8, half)
        one, two = (block[:, 0], block[:, 1])
        low = jnp.where(upper, one, pltpu.roll(two, 4, 1))
        high = jnp.where(upper, pltpu.roll(one, 4, 1), two)
        at = pl.ds(i * (group // 2), group // 2)
        rows_in[at, 0:half] = low.reshape(group // 2, half).astype(BF16)
        rows_in[at, half : 2 * half] = high.reshape(group // 2, half).astype(BF16)
        return carry

    lax.fori_loop(0, slots_ref.shape[0] // group, untangle, 0)

    rows = rows_in.shape[0] // 2
    for i in range(split):
        gate_copies[i].wait()
        up_copies[i].wait()
        for m in range(2):
            at = slice(m * rows, (m + 1) * rows)
            gates = dot_nn(rows_in[at, :], gate_in[i])
            ups = dot_nn(rows_in[at, :], up_in[i])
            hidden[at, cols[i]] = (gates / (1.0 + jnp.exp(-gates)) * ups).astype(BF16)

    top = lax.broadcasted_iota(jnp.int32, (rows // 8, 8, wide), 1) < 4
    for i in range(split):
        down_copies[i][0].wait()
        down_copies[i][1].wait()
        for m in range(2):
            at = slice(m * rows, (m + 1) * rows)
            low = dot_nn(hidden[at, :], down_in[i, 0]).reshape(-1, 8, wide)
            high = dot_nn(hidden[at, :], down_in[i, 1]).reshape(-1, 8, wide)
            one = jnp.where(top, low, pltpu.roll(high, 4, 1))
            two = jnp.where(top, pltpu.roll(low, 4, 1), high)
            both = jnp.stack([one, two], axis=1).reshape(2 * rows, wide).astype(BF16)
            outs[i, 2 * m * rows : 2 * (m + 1) * rows, :] = both
        out_copies[i].start()
    for i in range(split):
        out_copies[i].wait()


def experts_on(slots, gate_matrix, up_matrix, down_matrix):
    rows, half = slots.shape
    width, inner = gate_matrix.shape[1:]
    split = 4
    wide = inner // split
    there = pl.BlockSpec(memory_space=pl.ANY)
    return pl.pallas_call(
        expert_kernel,
        in_specs=[pl.BlockSpec((rows, half), lambda: (0, 0)), there, there, there],
        out_specs=there,
        out_shape=pltpu.HBM((rows, half), BF16),
        scratch_shapes=[
            pltpu.VMEM((rows // 2, width), BF16),
            pltpu.VMEM((rows // 2, inner), BF16),
            pltpu.VMEM((split, width, wide), BF16),
            pltpu.VMEM((split, width, wide), BF16),
            pltpu.VMEM((split, 2, inner, half // split), BF16),
            pltpu.VMEM((split, rows, half // split), BF16),
            pltpu.SemaphoreType.DMA((5, split)),
        ],
        compiler_params=params(40),
        name="experts_on",
    )(slots, in_hbm(gate_matrix), in_hbm(up_matrix), in_hbm(down_matrix))


def combine_kernel(returned_ref, pick_ref, stream_ref, weight_ref, out_ref):
    rows, width = out_ref.shape
    half = returned_ref.shape[1]
    weights = weight_ref[...]
    wide = 256
    for n in range(half // wide):
        picked = dot_nn(pick_ref[...], returned_ref[:, n * wide : (n + 1) * wide])
        for j in range(2):
            at = 2 * j * rows
            cols = slice(j * half + n * wide, j * half + (n + 1) * wide)
            added = weights[:, 0:1] * picked[at : at + rows] + weights[:, 1:2] * picked[at + rows : at + 2 * rows]
            out_ref[:, cols] = (stream_ref[:, cols].astype(F32) + added).astype(BF16)


def combine(returned, pick, stream, routing_weight):
    return pl.pallas_call(
        combine_kernel,
        out_shape=jax.ShapeDtypeStruct(stream.shape, BF16),
        compiler_params=params(24),
        name="combine",
    )(returned, pick, in_hbm(stream), routing_weight)


def body(
    resid,
    query,
    forget_logits,
    forget_margin,
    decay_spike,
    value_logits,
    output_gate_logits,
    head_norm_scale,
    output_matrix,
    norm_scale_vector,
    routes,
    routing_weight,
    gate_matrix,
    up_matrix,
    down_matrix,
):
    rows, top = routes.shape
    experts = lax.axis_size(SP) * lax.axis_size("tp")
    capacity = 2 * rows * top // experts
    width = resid.shape[1]
    margin = forget_margin[None, :]
    places = lax.axis_size("tp")
    place = lax.axis_index("tp").astype(jnp.int32)[None]
    cum, values, start, sent = local_states(forget_logits, value_logits, margin, decay_spike.T)
    parts = lax.all_to_all(sent, SP, split_axis=0, concat_axis=0, tiled=True)
    within, high, low, gates = within_blocks(
        query, forget_logits, margin, cum, values, start, output_gate_logits, head_norm_scale[None, :]
    )
    prior = lax.all_to_all(carried_in(parts), SP, split_axis=0, concat_axis=0, tiled=True)
    gated = gated_rows(place, within, high, low, prior.reshape(start.shape[1], DK), gates)
    shifts = (1, places - 1, 2)
    sent_on = {
        k: lax.ppermute(gated[k], "tp", [(i, (i + k) % places) for i in range(places)]) for k in (2, 1, places - 1)
    }
    own, select, pick = project_own(place, gated[0], output_matrix, resid, routes, experts, capacity)
    stream, packed = project(
        place, [sent_on[k] for k in shifts], shifts, output_matrix, own, norm_scale_vector[None, :], select
    )
    shape = (experts, 2 * capacity, width // 2)
    slots = lax.all_to_all(packed.reshape(shape), SP_TP, split_axis=0, concat_axis=0, tiled=True)
    answers = experts_on(slots.reshape(packed.shape), gate_matrix, up_matrix, down_matrix)
    returned = lax.all_to_all(answers.reshape(shape), SP_TP, split_axis=0, concat_axis=0, tiled=True)
    return combine(returned.reshape(packed.shape), pick, stream, routing_weight)


def solution(mesh):
    finer = Mesh(mesh.devices.reshape(4, 4, 2, mesh.shape["tp"]), SP_TP)
    placed = (
        P(SP_TP, None),
        P(SP, "tp"),
        P(SP, "tp"),
        P("tp"),
        P(SP, "tp"),
        P(SP, "tp"),
        P(SP, "tp"),
        P("tp"),
        P(),
        P(),
        P(SP_TP, None),
        P(SP_TP, None),
        P(SP_TP, None, None),
        P(SP_TP, None, None),
        P(SP_TP, None, None),
    )
    return jax.shard_map(
        body, mesh=finer, in_specs=placed, out_specs=P(SP_TP, None), check_vma=False
    )
```

```python
import functools

import jax
import jax.numpy as jnp
from jax import lax
from jax.experimental import pallas as pl
from jax.experimental.pallas import tpu as pltpu
from jax.sharding import Mesh
from jax.sharding import PartitionSpec as P

DK = 128
CHUNK = 128
SP = ("sp_0", "sp_1", "sp_2")
SP_TP = ("sp_0", "sp_1", "sp_2", "tp")
F32 = jnp.float32
BF16 = jnp.bfloat16


def dot_nn(a, b):
    return lax.dot_general(a, b, (((1,), (0,)), ((), ())), preferred_element_type=F32)


def dot_nt(a, b):
    return lax.dot_general(a, b, (((1,), (1,)), ((), ())), preferred_element_type=F32)


def dot_tn(a, b):
    return lax.dot_general(a, b, (((0,), (0,)), ((), ())), preferred_element_type=F32)


def lower_mask(n, strict):
    row = lax.broadcasted_iota(jnp.int32, (n, n), 0)
    col = lax.broadcasted_iota(jnp.int32, (n, n), 1)
    return row > col if strict else row >= col


def in_hbm(value):
    return pltpu.with_memory_space_constraint(value, pltpu.HBM)


def in_vmem(value):
    return pltpu.with_memory_space_constraint(value, pltpu.VMEM)


def params(mebibytes):
    return pltpu.CompilerParams(vmem_limit_bytes=mebibytes * 1024 * 1024)


def halves(value):
    high = value.astype(BF16)
    return high, (value - high.astype(F32)).astype(BF16)


def state_kernel(forget_ref, value_ref, margin_ref, spike_ref, cum_ref, values_ref, start_ref, sent_ref, state, before):
    step = pl.program_id(0)
    heads = forget_ref.shape[1] // DK

    @pl.when(step == 0)
    def _():
        state[...] = jnp.zeros_like(state)
        before[...] = jnp.zeros_like(before)

    tri = lower_mask(CHUNK, False).astype(BF16)
    for c in range(forget_ref.shape[0] // CHUNK):
        rows = slice(c * CHUNK, (c + 1) * CHUNK)
        spikes = halves(spike_ref[:, rows])
        spikes = dot_nt(tri, spikes[0]) + dot_nt(tri, spikes[1])
        start_ref[c] = state[...]
        for h in range(heads):
            cols = slice(h * DK, (h + 1) * DK)
            keys = margin_ref[:, cols] / (1.0 + jnp.exp(forget_ref[rows, cols].astype(F32)))
            high, low = halves(jnp.log(1.0 - keys))
            cum = dot_nn(tri, high) + dot_nn(tri, low) + spikes[:, h : h + 1]
            cum_ref[rows, cols] = cum
            last = cum[CHUNK - 1 : CHUNK, :]
            logits = value_ref[rows, cols].astype(F32)
            values = (logits / (1.0 + jnp.exp(-logits))).astype(BF16)
            values_ref[rows, cols] = values
            kept = (keys * jnp.exp(last - cum)).astype(BF16)
            state[cols, :] = jnp.exp(last) * state[cols, :] + dot_tn(values, kept)
            before[:, cols] = before[:, cols] + last

    @pl.when(step == pl.num_programs(0) - 1)
    def _():
        share = DK // 8
        first = lax.broadcasted_iota(jnp.int32, (share, DK), 0) == 0
        for h in range(heads):
            total = before[:, h * DK : (h + 1) * DK]
            high = total.astype(BF16).astype(F32)
            tail = jnp.where(first, high, total - high).astype(BF16)
            for i in range(8):
                row = h * DK + i * share
                sent_ref[h * 8 + i, 0:share, :] = state[row : row + share, :].astype(BF16)
                sent_ref[h * 8 + i, share : 2 * share, :] = tail


STATE_STEPS = 2


def local_states(forget_logits, value_logits, margin, spike):
    rows, width = forget_logits.shape
    heads = width // DK
    size = rows // STATE_STEPS
    by_rows = lambda i: (i, 0)
    return pl.pallas_call(
        state_kernel,
        grid=(STATE_STEPS,),
        in_specs=[
            pl.BlockSpec((size, width), by_rows),
            pl.BlockSpec((size, width), by_rows),
            pl.BlockSpec((1, width), lambda i: (0, 0)),
            pl.BlockSpec((heads, size), lambda i: (0, i)),
        ],
        out_specs=[
            pl.BlockSpec((size, width), by_rows),
            pl.BlockSpec((size, width), by_rows),
            pl.BlockSpec((size // CHUNK, width, DK), lambda i: (i, 0, 0)),
            pl.BlockSpec((heads * 8, 2 * DK // 8, DK), lambda i: (0, 0, 0)),
        ],
        out_shape=[
            pltpu.HBM((rows, width), F32),
            pltpu.HBM((rows, width), BF16),
            pltpu.HBM((rows // CHUNK, width, DK), F32),
            pltpu.HBM((heads * 8, 2 * DK // 8, DK), BF16),
        ],
        scratch_shapes=[pltpu.VMEM((width, DK), F32), pltpu.VMEM((1, width), F32)],
        compiler_params=params(16),
        name="local_states",
    )(*map(in_hbm, (forget_logits, value_logits, margin, spike)))


def carry_kernel(parts_ref, prior_ref):
    share = prior_ref.shape[1]
    running = jnp.zeros(prior_ref.shape[1:], F32)
    for d in range(parts_ref.shape[0]):
        prior_ref[d] = running
        tail = parts_ref[d, share : 2 * share, :].astype(F32)
        total = tail[0:1, :] + tail[1:2, :]
        running = jnp.exp(total) * running + parts_ref[d, 0:share, :].astype(F32)


def carried_in(parts):
    return pl.pallas_call(
        carry_kernel,
        out_shape=jax.ShapeDtypeStruct((parts.shape[0], parts.shape[1] // 2, parts.shape[2]), F32),
        compiler_params=params(8),
        name="carried_in",
    )(parts)


def dot_split(queries, states):
    return dot_nt(queries[0], states[0]) + dot_nt(queries[0], states[1]) + dot_nt(queries[1], states[0])


def within_kernel(query_ref, forget_ref, margin_ref, cum_ref, values_ref, start_ref, gate_ref, scale_ref, out_ref, high_ref, low_ref, gates_ref, before):
    heads = query_ref.shape[1] // DK
    causal = lower_mask(CHUNK, False)

    @pl.when(pl.program_id(0) == 0)
    def _():
        before[...] = jnp.zeros_like(before)

    for h in range(heads):
        cols = slice(h * DK, (h + 1) * DK)
        cum = cum_ref[:, cols]
        spread = cum - cum[CHUNK // 2 - 1 : CHUNK // 2, :]
        keys = margin_ref[:, cols] / (1.0 + jnp.exp(forget_ref[:, cols].astype(F32)))
        queries = query_ref[:, cols].astype(F32) * (DK**-0.5)
        scores = dot_nt((queries * jnp.exp(spread)).astype(BF16), (keys * jnp.exp(-spread)).astype(BF16))
        scores = jnp.where(causal, scores, 0.0).astype(BF16)
        decayed = queries * jnp.exp(cum)
        earlier = dot_split(halves(decayed), halves(start_ref[0, cols, :]))
        out_ref[:, cols] = dot_nn(scores, values_ref[:, cols]) + earlier
        high_ref[:, cols], low_ref[:, cols] = halves(decayed * jnp.exp(before[:, cols]))
        before[:, cols] = before[:, cols] + cum[CHUNK - 1 : CHUNK, :]
        logits = gate_ref[:, cols].astype(F32)
        gates_ref[:, cols] = scale_ref[:, cols] * (logits / (1.0 + jnp.exp(-logits)))


def within_blocks(query, forget_logits, margin, cum, values, start, gate_logits, scale):
    rows, width = query.shape
    block = pl.BlockSpec((CHUNK, width), lambda i: (i, 0))
    row = pl.BlockSpec((1, width), lambda i: (0, 0))
    return pl.pallas_call(
        within_kernel,
        grid=(rows // CHUNK,),
        in_specs=[block, block, row, block, block, pl.BlockSpec((1, width, DK), lambda i: (i, 0, 0)), block, row],
        out_specs=[block, block, block, block],
        out_shape=[pltpu.VMEM((rows, width), kind) for kind in (F32, BF16, BF16, F32)],
        scratch_shapes=[pltpu.VMEM((1, width), F32)],
        compiler_params=params(24),
        name="within_blocks",
    )(*map(in_hbm, (query, forget_logits, margin, cum, values, start, gate_logits, scale)))


def readout_kernel(within_ref, high_ref, low_ref, prior_ref, gates_ref, out_ref, *, shift):
    heads = within_ref.shape[1] // DK
    blocks = within_ref.shape[0] // CHUNK
    rows = pl.ds((lax.axis_index("tp") + shift) % blocks * CHUNK, CHUNK)
    for h in range(heads):
        cols = slice(h * DK, (h + 1) * DK)
        carried = dot_split((high_ref[rows, cols], low_ref[rows, cols]), halves(prior_ref[cols, :]))
        recurrent = within_ref[rows, cols] + carried
        square = jnp.mean(recurrent * recurrent, axis=1, keepdims=True)
        out_ref[:, cols] = (recurrent * lax.rsqrt(square + 1e-06) * gates_ref[rows, cols]).astype(BF16)


def gated_rows(shift, within, high, low, prior, gates):
    here = pl.BlockSpec(memory_space=pltpu.VMEM)
    return pl.pallas_call(
        functools.partial(readout_kernel, shift=shift),
        in_specs=[here] * 5,
        out_specs=here,
        out_shape=pltpu.VMEM((CHUNK, within.shape[1]), BF16),
        compiler_params=params(16),
        name="gated_rows",
    )(*map(in_vmem, (within, high, low, prior, gates)))


def slot_positions(routes, experts, capacity):
    rows = routes.shape[0]
    lanes = lax.broadcasted_iota(jnp.int32, (rows, experts), 1)
    first, second = (routes[:, 0:1], routes[:, 1:2])
    one, two = (lanes == first, lanes == second)
    named = (one.astype(F32) + two.astype(F32)).astype(BF16)
    earlier = dot_nn(lower_mask(rows, True).astype(BF16), named)
    ranks = [
        jnp.sum(jnp.where(hit, earlier, 0.0), axis=1, keepdims=True).astype(jnp.int32)
        for hit in (one, two)
    ]
    return [expert * (2 * capacity) + rank for expert, rank in zip((first, second), ranks)]


def slots_kernel(routes_ref, select_ref, pick_ref, *, experts, capacity):
    rows = routes_ref.shape[0]
    slots = 2 * experts * capacity
    places = slot_positions(routes_ref[...], experts, capacity)
    lanes = lax.broadcasted_iota(jnp.int32, (rows, slots), 1)
    down = lax.broadcasted_iota(jnp.int32, (slots, rows), 0)
    across = [
        jnp.transpose(jnp.broadcast_to(place.astype(F32), (rows, rows)))[0:1, :].astype(jnp.int32)
        for place in places
    ]
    for j in range(2):
        hit = (down == across[0] + j * capacity) | (down == across[1] + j * capacity)
        select_ref[:, j * rows : (j + 1) * rows] = jnp.where(hit, 1.0, 0.0).astype(BF16)
        for k in range(2):
            at = (2 * j + k) * rows
            pick_ref[at : at + rows, :] = jnp.where(lanes == places[k] + j * capacity, 1.0, 0.0).astype(BF16)


def slots_of(routes, experts, capacity):
    rows = routes.shape[0]
    slots = 2 * experts * capacity
    return pl.pallas_call(
        functools.partial(slots_kernel, experts=experts, capacity=capacity),
        out_shape=[pltpu.HBM((slots, 2 * rows), BF16), pltpu.HBM((4 * rows, slots), BF16)],
        compiler_params=params(12),
        name="slots_of",
    )(routes)


def own_kernel(own_ref, matrix_ref, resid_ref, select_ref, total_ref, matrix_out_ref, select_out_ref, sems):
    place = lax.axis_index("tp")
    inner = own_ref.shape[1]
    parts = sems.shape[0] - 1
    copies = []
    for k in range(parts):
        at = pl.ds((place + k) % parts * inner, inner)
        copies.append(pltpu.make_async_copy(matrix_ref.at[at, :], matrix_out_ref.at[at, :], sems.at[k]))
    copies.append(pltpu.make_async_copy(select_ref, select_out_ref, sems.at[parts]))
    for copy in copies:
        copy.start()
    copies[0].wait()
    part = dot_nn(own_ref[...], matrix_out_ref[pl.ds(place * inner, inner), :])
    total_ref[...] = resid_ref[...].astype(F32) + part
    for copy in copies[1:]:
        copy.wait()


def project_own(own, matrix, resid, select):
    rows = own.shape[0]
    here = pl.BlockSpec(memory_space=pltpu.VMEM)
    there = pl.BlockSpec(memory_space=pl.ANY)
    return pl.pallas_call(
        own_kernel,
        in_specs=[here, there, here, there],
        out_specs=[here, here, here],
        out_shape=[
            pltpu.VMEM((rows, matrix.shape[1]), F32),
            pltpu.VMEM(matrix.shape, BF16),
            pltpu.VMEM(select.shape, BF16),
        ],
        scratch_shapes=[pltpu.SemaphoreType.DMA((matrix.shape[0] // own.shape[1] + 1,))],
        compiler_params=params(16),
        name="project_own",
    )(in_vmem(own), in_hbm(matrix), in_vmem(resid), in_hbm(select))


def add_part(total, part_ref, matrix_ref, shift):
    inner = part_ref.shape[1]
    parts = matrix_ref.shape[0] // inner
    source = (lax.axis_index("tp") + parts - shift) % parts
    return total + dot_nn(part_ref[...], matrix_ref[pl.ds(source * inner, inner), :])


def more_kernel(part_ref, matrix_ref, total_ref, out_ref, *, shift):
    out_ref[...] = add_part(total_ref[...], part_ref, matrix_ref, shift)


def project_more(part, shift, matrix, total):
    here = pl.BlockSpec(memory_space=pltpu.VMEM)
    return pl.pallas_call(
        functools.partial(more_kernel, shift=shift),
        in_specs=[here, here, here],
        out_specs=here,
        out_shape=pltpu.VMEM(total.shape, F32),
        compiler_params=params(16),
        name="project_more",
    )(*map(in_vmem, (part, matrix, total)))


def project_kernel(part_ref, matrix_ref, total_ref, scale_ref, select_ref, stream_ref, packed_ref, stream_out, stacked, sem, *, shift):
    stream = add_part(total_ref[...], part_ref, matrix_ref, shift).astype(BF16)
    stream_out[...] = stream
    stream_copy = pltpu.make_async_copy(stream_out, stream_ref, sem)
    stream_copy.start()
    values = stream.astype(F32)
    square = jnp.mean(values * values, axis=1, keepdims=True)
    normed = (values * lax.rsqrt(square + 1e-06) * scale_ref[...]).astype(BF16)
    rows = normed.shape[0]
    half = normed.shape[1] // 2
    stacked[0:rows, :] = normed[:, :half]
    stacked[rows : 2 * rows, :] = normed[:, half:]
    packed_ref[...] = dot_nn(select_ref[...], stacked[...]).astype(BF16)
    stream_copy.wait()


def project(part, shift, matrix, total, scale, select):
    rows, width = total.shape
    slots = select.shape[0]
    here = pl.BlockSpec(memory_space=pltpu.VMEM)
    return pl.pallas_call(
        functools.partial(project_kernel, shift=shift),
        in_specs=[here, here, here, pl.BlockSpec((1, width), lambda: (0, 0)), here],
        out_specs=[pl.BlockSpec(memory_space=pl.ANY), here],
        scratch_shapes=[
            pltpu.VMEM((rows, width), BF16),
            pltpu.VMEM((2 * rows, width // 2), BF16),
            pltpu.SemaphoreType.DMA,
        ],
        out_shape=[pltpu.HBM((rows, width), BF16), pltpu.VMEM((slots, width // 2), BF16)],
        compiler_params=params(24),
        name="project",
    )(in_vmem(part), in_vmem(matrix), in_vmem(total), in_hbm(scale), in_vmem(select))


def expert_kernel(slots_ref, gate_ref, up_ref, down_ref, out_ref, rows_in, hidden, outs, sems):
    half = slots_ref.shape[1]
    split, rows2, wide = outs.shape
    rows = rows2 // 2
    cols = [slice(i * wide, (i + 1) * wide) for i in range(split)]
    out_copies = [pltpu.make_async_copy(outs.at[i], out_ref.at[:, cols[i]], sems.at[i]) for i in range(split)]
    group = 64
    upper = lax.broadcasted_iota(jnp.int32, (group // 16, 8, half), 1) < 4

    def untangle(i, carry):
        block = slots_ref[pl.ds(i * group, group), :].astype(F32).reshape(group // 16, 2, 8, half)
        one, two = (block[:, 0], block[:, 1])
        low = jnp.where(upper, one, pltpu.roll(two, 4, 1))
        high = jnp.where(upper, pltpu.roll(one, 4, 1), two)
        at = pl.ds(i * (group // 2), group // 2)
        rows_in[at, 0:half] = low.reshape(group // 2, half).astype(BF16)
        rows_in[at, half : 2 * half] = high.reshape(group // 2, half).astype(BF16)
        return carry

    lax.fori_loop(0, slots_ref.shape[0] // group, untangle, 0)

    for i in range(split):
        gates = dot_nn(rows_in[...], gate_ref[0, :, cols[i]])
        ups = dot_nn(rows_in[...], up_ref[0, :, cols[i]])
        hidden[:, cols[i]] = (gates / (1.0 + jnp.exp(-gates)) * ups).astype(BF16)

    top = lax.broadcasted_iota(jnp.int32, (rows // 8, 8, wide), 1) < 4
    for i in range(split):
        low = dot_nn(hidden[...], down_ref[0, :, cols[i]]).reshape(-1, 8, wide)
        high = dot_nn(hidden[...], down_ref[0, :, half + i * wide : half + (i + 1) * wide]).reshape(-1, 8, wide)
        one = jnp.where(top, low, pltpu.roll(high, 4, 1))
        two = jnp.where(top, pltpu.roll(low, 4, 1), high)
        outs[i] = jnp.stack([one, two], axis=1).reshape(2 * rows, wide).astype(BF16)
        out_copies[i].start()
    for i in range(split):
        out_copies[i].wait()


def experts_on(slots, gate_matrix, up_matrix, down_matrix):
    rows, half = slots.shape
    width, inner = gate_matrix.shape[1:]
    split = 4
    here = pl.BlockSpec(memory_space=pltpu.VMEM)
    return pl.pallas_call(
        expert_kernel,
        in_specs=[here, here, here, here],
        out_specs=pl.BlockSpec(memory_space=pl.ANY),
        out_shape=pltpu.HBM((rows, half), BF16),
        scratch_shapes=[
            pltpu.VMEM((rows // 2, width), BF16),
            pltpu.VMEM((rows // 2, inner), BF16),
            pltpu.VMEM((split, rows, half // split), BF16),
            pltpu.SemaphoreType.DMA((split,)),
        ],
        compiler_params=params(24),
        name="experts_on",
    )(*map(in_vmem, (slots, gate_matrix, up_matrix, down_matrix)))


def combine_kernel(returned_ref, pick_ref, weight_ref, stream_ref, out_ref, stream_in, outs, sems):
    rows, _ = stream_in.shape
    half = returned_ref.shape[1]
    stream_copy = pltpu.make_async_copy(stream_ref, stream_in, sems.at[0])
    stream_copy.start()
    weights = weight_ref[...]
    wide = outs.shape[2]
    copies = []
    for n in range(half // wide):
        picked = dot_nn(pick_ref[...], returned_ref[:, n * wide : (n + 1) * wide])
        if n == 0:
            stream_copy.wait()
        for j in range(2):
            at = 2 * j * rows
            cols = slice(j * half + n * wide, j * half + (n + 1) * wide)
            added = weights[:, 0:1] * picked[at : at + rows] + weights[:, 1:2] * picked[at + rows : at + 2 * rows]
            slot = 2 * n + j
            outs[slot] = (stream_in[:, cols].astype(F32) + added).astype(BF16)
            copies.append(pltpu.make_async_copy(outs.at[slot], out_ref.at[:, cols], sems.at[slot + 1]))
            copies[-1].start()
    for copy in copies:
        copy.wait()


def combine(returned, pick, stream, routing_weight):
    rows, width = stream.shape
    here = pl.BlockSpec(memory_space=pltpu.VMEM)
    there = pl.BlockSpec(memory_space=pl.ANY)
    pieces = 8
    return pl.pallas_call(
        combine_kernel,
        in_specs=[here, here, here, there],
        out_specs=there,
        out_shape=pltpu.HBM(stream.shape, BF16),
        scratch_shapes=[
            pltpu.VMEM((rows, width), BF16),
            pltpu.VMEM((pieces, rows, width // pieces), BF16),
            pltpu.SemaphoreType.DMA((pieces + 1,)),
        ],
        compiler_params=params(24),
        name="combine",
    )(in_vmem(returned), in_vmem(pick), in_vmem(routing_weight), in_hbm(stream))


def body(
    resid,
    query,
    forget_logits,
    forget_margin,
    decay_spike,
    value_logits,
    output_gate_logits,
    head_norm_scale,
    output_matrix,
    norm_scale_vector,
    routes,
    routing_weight,
    gate_matrix,
    up_matrix,
    down_matrix,
):
    rows, top = routes.shape
    experts = lax.axis_size(SP) * lax.axis_size("tp")
    capacity = 2 * rows * top // experts
    width = resid.shape[1]
    margin = forget_margin[None, :]
    places = lax.axis_size("tp")
    cum, values, start, sent = local_states(forget_logits, value_logits, margin, decay_spike.T)
    select, pick = slots_of(routes, experts, capacity)
    parts = lax.all_to_all(sent, SP, split_axis=0, concat_axis=0, tiled=True)
    within, high, low, gates = within_blocks(
        query, forget_logits, margin, cum, values, start, output_gate_logits, head_norm_scale[None, :]
    )
    prior = lax.all_to_all(carried_in(parts), SP, split_axis=0, concat_axis=0, tiled=True)
    prior = prior.reshape(start.shape[1], DK)
    shifts = (2, 1, places - 1)
    arrived = []
    for k in shifts + (0,):
        gated = gated_rows(k, within, high, low, prior, gates)
        if k:
            arrived.append(lax.ppermute(gated, "tp", [(i, (i + k) % places) for i in range(places)]))
    total, matrix, select = project_own(gated, output_matrix, resid, select)
    total = project_more(arrived[0], shifts[0], matrix, total)
    total = project_more(arrived[1], shifts[1], matrix, total)
    stream, packed = project(arrived[2], shifts[2], matrix, total, norm_scale_vector[None, :], select)
    shape = (experts, 2 * capacity, width // 2)
    slots = lax.all_to_all(packed.reshape(shape), SP_TP, split_axis=0, concat_axis=0, tiled=True)
    answers = experts_on(slots.reshape(packed.shape), gate_matrix, up_matrix, down_matrix)
    returned = lax.all_to_all(answers.reshape(shape), SP_TP, split_axis=0, concat_axis=0, tiled=True)
    return combine(returned.reshape(packed.shape), pick, stream, routing_weight)


def solution(mesh):
    finer = Mesh(mesh.devices.reshape(4, 4, 2, mesh.shape["tp"]), SP_TP)
    placed = (
        P(SP_TP, None),
        P(SP, "tp"),
        P(SP, "tp"),
        P("tp"),
        P(SP, "tp"),
        P(SP, "tp"),
        P(SP, "tp"),
        P("tp"),
        P(),
        P(),
        P(SP_TP, None),
        P(SP_TP, None),
        P(SP_TP, None, None),
        P(SP_TP, None, None),
        P(SP_TP, None, None),
    )
    return jax.shard_map(
        body, mesh=finer, in_specs=placed, out_specs=P(SP_TP, None), check_vma=False
    )
```

```python
import functools

import jax
import jax.numpy as jnp
from jax import lax
from jax.experimental import pallas as pl
from jax.experimental.pallas import tpu as pltpu
from jax.sharding import Mesh
from jax.sharding import PartitionSpec as P

DK = 128
CHUNK = 128
SP = ("sp_0", "sp_1", "sp_2")
SP_TP = ("sp_0", "sp_1", "sp_2", "tp")
F32 = jnp.float32
BF16 = jnp.bfloat16


def dot_nn(a, b):
    return lax.dot_general(a, b, (((1,), (0,)), ((), ())), preferred_element_type=F32)


def dot_nt(a, b):
    return lax.dot_general(a, b, (((1,), (1,)), ((), ())), preferred_element_type=F32)


def dot_tn(a, b):
    return lax.dot_general(a, b, (((0,), (0,)), ((), ())), preferred_element_type=F32)


def lower_mask(n, strict):
    row = lax.broadcasted_iota(jnp.int32, (n, n), 0)
    col = lax.broadcasted_iota(jnp.int32, (n, n), 1)
    return row > col if strict else row >= col


def in_hbm(value):
    return pltpu.with_memory_space_constraint(value, pltpu.HBM)


def in_vmem(value):
    return pltpu.with_memory_space_constraint(value, pltpu.VMEM)


def params(mebibytes):
    return pltpu.CompilerParams(vmem_limit_bytes=mebibytes * 1024 * 1024)


def sigmoid(value):
    return 1.0 / (1.0 + jnp.exp(-value))


def halves(value):
    high = value.astype(BF16)
    return high, (value - high.astype(F32)).astype(BF16)


def state_kernel(forget_ref, value_ref, margin_ref, spike_ref, cum_ref, values_ref, start_ref, sent_ref, state, before, keys_in, decays):
    step = pl.program_id(0)
    heads = forget_ref.shape[1] // DK

    @pl.when(step == 0)
    def _():
        state[...] = jnp.zeros_like(state)
        before[...] = jnp.zeros_like(before)

    tri = lower_mask(CHUNK, False).astype(BF16)
    tri = jnp.concatenate([tri, tri], axis=1)
    blocks = [slice(c * CHUNK, (c + 1) * CHUNK) for c in range(forget_ref.shape[0] // CHUNK)]
    for c, rows in enumerate(blocks):
        for h in range(heads):
            cols = slice(h * DK, (h + 1) * DK)
            keys = margin_ref[:, cols] * sigmoid(-forget_ref[rows, cols].astype(F32))
            keys_in[rows, cols] = keys
            decays[c, 0:CHUNK, cols], decays[c, CHUNK : 2 * CHUNK, cols] = halves(jnp.log(1.0 - keys))
    for c, rows in enumerate(blocks):
        spikes = dot_nt(tri, jnp.concatenate(halves(spike_ref[:, rows]), axis=1))
        sums = dot_nn(tri, decays[c])
        for h in range(heads):
            cols = slice(h * DK, (h + 1) * DK)
            cum_ref[rows, cols] = sums[:, cols] + spikes[:, h : h + 1]
    for c, rows in enumerate(blocks):
        start_ref[c] = state[...]
        for h in range(heads):
            cols = slice(h * DK, (h + 1) * DK)
            cum = cum_ref[rows, cols]
            last = cum[CHUNK - 1 : CHUNK, :]
            logits = value_ref[rows, cols].astype(F32)
            values = (logits * sigmoid(logits)).astype(BF16)
            values_ref[rows, cols] = values
            kept = (keys_in[rows, cols] * jnp.exp(last - cum)).astype(BF16)
            state[cols, :] = jnp.exp(last) * state[cols, :] + dot_tn(values, kept)
            before[:, cols] = before[:, cols] + last

    @pl.when(step == pl.num_programs(0) - 1)
    def _():
        share = DK // 8
        first = lax.broadcasted_iota(jnp.int32, (TAIL, DK), 0) == 0
        for h in range(heads):
            total = before[:, h * DK : (h + 1) * DK]
            high = total.astype(BF16).astype(F32)
            tail = jnp.where(first, high, total - high).astype(BF16)
            for i in range(8):
                row = h * DK + i * share
                sent_ref[h * 8 + i, 0:share, :] = state[row : row + share, :].astype(BF16)
                sent_ref[h * 8 + i, share : share + TAIL, :] = tail


STATE_STEPS = 2
TAIL = 8


def local_states(forget_logits, value_logits, margin, spike):
    rows, width = forget_logits.shape
    heads = width // DK
    size = rows // STATE_STEPS
    by_rows = lambda i: (i, 0)
    return pl.pallas_call(
        state_kernel,
        grid=(STATE_STEPS,),
        in_specs=[
            pl.BlockSpec((size, width), by_rows),
            pl.BlockSpec((size, width), by_rows),
            pl.BlockSpec((1, width), lambda i: (0, 0)),
            pl.BlockSpec((heads, size), lambda i: (0, i)),
        ],
        out_specs=[
            pl.BlockSpec((size, width), by_rows),
            pl.BlockSpec((size, width), by_rows),
            pl.BlockSpec((size // CHUNK, width, DK), lambda i: (i, 0, 0)),
            pl.BlockSpec((heads * 8, DK // 8 + TAIL, DK), lambda i: (0, 0, 0)),
        ],
        out_shape=[
            pltpu.HBM((rows, width), F32),
            pltpu.HBM((rows, width), BF16),
            pltpu.HBM((rows // CHUNK, width, DK), F32),
            pltpu.HBM((heads * 8, DK // 8 + TAIL, DK), BF16),
        ],
        scratch_shapes=[
            pltpu.VMEM((width, DK), F32),
            pltpu.VMEM((1, width), F32),
            pltpu.VMEM((size, width), F32),
            pltpu.VMEM((size // CHUNK, 2 * CHUNK, width), BF16),
        ],
        compiler_params=params(16),
        name="local_states",
    )(*map(in_hbm, (forget_logits, value_logits, margin, spike)))


def carry_kernel(parts_ref, prior_ref):
    share = prior_ref.shape[1]
    running = jnp.zeros(prior_ref.shape[1:], F32)
    for d in range(parts_ref.shape[0]):
        prior_ref[d] = running
        tail = parts_ref[d, share : share + TAIL, :].astype(F32)
        total = tail[0:1, :] + tail[1:2, :]
        running = jnp.exp(total) * running + parts_ref[d, 0:share, :].astype(F32)


def carried_in(parts):
    return pl.pallas_call(
        carry_kernel,
        out_shape=pltpu.HBM((parts.shape[0], parts.shape[1] - TAIL, parts.shape[2]), F32),
        compiler_params=params(8),
        name="carried_in",
    )(parts)


def dot_split(queries, states):
    return dot_nt(queries[0], states[0]) + dot_nt(queries[0], states[1]) + dot_nt(queries[1], states[0])


def within_kernel(query_ref, forget_ref, margin_ref, cum_ref, values_ref, start_ref, gate_ref, scale_ref, out_ref, high_ref, low_ref, gates_ref, before):
    heads = query_ref.shape[1] // DK
    causal = lower_mask(CHUNK, False)

    @pl.when(pl.program_id(0) == 0)
    def _():
        before[...] = jnp.zeros_like(before)

    for h in range(heads):
        cols = slice(h * DK, (h + 1) * DK)
        cum = cum_ref[:, cols]
        spread = cum - cum[CHUNK // 2 - 1 : CHUNK // 2, :]
        keys = margin_ref[:, cols] * sigmoid(-forget_ref[:, cols].astype(F32))
        queries = query_ref[:, cols].astype(F32) * (DK**-0.5)
        scores = dot_nt((queries * jnp.exp(spread)).astype(BF16), (keys * jnp.exp(-spread)).astype(BF16))
        scores = jnp.where(causal, scores, 0.0).astype(BF16)
        decayed = queries * jnp.exp(cum)
        earlier = dot_split(halves(decayed), halves(start_ref[0, cols, :]))
        out_ref[:, cols] = dot_nn(scores, values_ref[:, cols]) + earlier
        high_ref[:, cols], low_ref[:, cols] = halves(decayed * jnp.exp(before[:, cols]))
        before[:, cols] = before[:, cols] + cum[CHUNK - 1 : CHUNK, :]
        logits = gate_ref[:, cols].astype(F32)
        gates_ref[:, cols] = scale_ref[:, cols] * (logits * sigmoid(logits))


def within_blocks(query, forget_logits, margin, cum, values, start, gate_logits, scale):
    rows, width = query.shape
    block = pl.BlockSpec((CHUNK, width), lambda i: (i, 0))
    row = pl.BlockSpec((1, width), lambda i: (0, 0))
    return pl.pallas_call(
        within_kernel,
        grid=(rows // CHUNK,),
        in_specs=[block, block, row, block, block, pl.BlockSpec((1, width, DK), lambda i: (i, 0, 0)), block, row],
        out_specs=[block, block, block, block],
        out_shape=[pltpu.VMEM((rows, width), kind) for kind in (F32, BF16, BF16, F32)],
        scratch_shapes=[pltpu.VMEM((1, width), F32)],
        compiler_params=params(24),
        name="within_blocks",
    )(*map(in_hbm, (query, forget_logits, margin, cum, values, start, gate_logits, scale)))


def readout(within_ref, high_ref, low_ref, prior_ref, gates_ref, out_ref, shift):
    heads = within_ref.shape[1] // DK
    blocks = within_ref.shape[0] // CHUNK
    rows = pl.ds((lax.axis_index("tp") + shift) % blocks * CHUNK, CHUNK)
    for h in range(heads):
        cols = slice(h * DK, (h + 1) * DK)
        carried = dot_split((high_ref[rows, cols], low_ref[rows, cols]), halves(prior_ref[cols, :]))
        recurrent = within_ref[rows, cols] + carried
        square = jnp.mean(recurrent * recurrent, axis=1, keepdims=True)
        out_ref[:, cols] = (recurrent * lax.rsqrt(square + 1e-06) * gates_ref[rows, cols]).astype(BF16)


def readout_kernel(*refs, shift):
    readout(*refs, shift)


def gated_rows(shift, within, high, low, prior, gates):
    here = pl.BlockSpec(memory_space=pltpu.VMEM)
    return pl.pallas_call(
        functools.partial(readout_kernel, shift=shift),
        in_specs=[here] * 5,
        out_specs=here,
        out_shape=pltpu.VMEM((CHUNK, within.shape[1]), BF16),
        compiler_params=params(16),
        name="gated_rows",
    )(*map(in_vmem, (within, high, low, prior, gates)))


def slot_positions(routes, experts, capacity):
    rows = routes.shape[0]
    lanes = lax.broadcasted_iota(jnp.int32, (rows, experts), 1)
    first, second = (routes[:, 0:1], routes[:, 1:2])
    one, two = (lanes == first, lanes == second)
    named = (one.astype(F32) + two.astype(F32)).astype(BF16)
    earlier = dot_nn(lower_mask(rows, True).astype(BF16), named)
    ranks = [
        jnp.sum(jnp.where(hit, earlier, 0.0), axis=1, keepdims=True).astype(jnp.int32)
        for hit in (one, two)
    ]
    return [expert * (2 * capacity) + rank for expert, rank in zip((first, second), ranks)]


def slots_kernel(routes_ref, select_ref, pick_ref, *, experts, capacity):
    rows = routes_ref.shape[0]
    slots = 2 * experts * capacity
    places = slot_positions(routes_ref[...], experts, capacity)
    lanes = lax.broadcasted_iota(jnp.int32, (rows, slots), 1)
    down = lax.broadcasted_iota(jnp.int32, (slots, rows), 0)
    across = [
        jnp.transpose(jnp.broadcast_to(place.astype(F32), (rows, rows)))[0:1, :].astype(jnp.int32)
        for place in places
    ]
    for j in range(2):
        hit = (down == across[0] + j * capacity) | (down == across[1] + j * capacity)
        select_ref[:, j * rows : (j + 1) * rows] = jnp.where(hit, 1.0, 0.0).astype(BF16)
        for k in range(2):
            at = (2 * j + k) * rows
            pick_ref[at : at + rows, :] = jnp.where(lanes == places[k] + j * capacity, 1.0, 0.0).astype(BF16)


def slots_of(routes, experts, capacity):
    rows = routes.shape[0]
    slots = 2 * experts * capacity
    return pl.pallas_call(
        functools.partial(slots_kernel, experts=experts, capacity=capacity),
        out_shape=[pltpu.HBM((slots, 2 * rows), BF16), pltpu.HBM((4 * rows, slots), BF16)],
        compiler_params=params(12),
        name="slots_of",
    )(routes)


def own_kernel(within_ref, high_ref, low_ref, prior_ref, gates_ref, matrix_ref, resid_ref, select_ref, total_ref, matrix_out_ref, select_out_ref, own, sems):
    place = lax.axis_index("tp")
    inner = own.shape[1]
    parts = sems.shape[0] - 1
    copies = []
    for k in range(parts):
        at = pl.ds((place + k) % parts * inner, inner)
        copies.append(pltpu.make_async_copy(matrix_ref.at[at, :], matrix_out_ref.at[at, :], sems.at[k]))
    copies.append(pltpu.make_async_copy(select_ref, select_out_ref, sems.at[parts]))
    for copy in copies:
        copy.start()
    readout(within_ref, high_ref, low_ref, prior_ref, gates_ref, own, 0)
    copies[0].wait()
    part = dot_nn(own[...], matrix_out_ref[pl.ds(place * inner, inner), :])
    total_ref[...] = resid_ref[...].astype(F32) + part
    for copy in copies[1:]:
        copy.wait()


def project_own(within, high, low, prior, gates, matrix, resid, select):
    here = pl.BlockSpec(memory_space=pltpu.VMEM)
    there = pl.BlockSpec(memory_space=pl.ANY)
    inner = within.shape[1]
    return pl.pallas_call(
        own_kernel,
        in_specs=[here, here, here, here, here, there, here, there],
        out_specs=[here, here, here],
        out_shape=[
            pltpu.VMEM(resid.shape, F32),
            pltpu.VMEM(matrix.shape, BF16),
            pltpu.VMEM(select.shape, BF16),
        ],
        scratch_shapes=[
            pltpu.VMEM((CHUNK, inner), BF16),
            pltpu.SemaphoreType.DMA((matrix.shape[0] // inner + 1,)),
        ],
        compiler_params=params(16),
        name="project_own",
    )(*map(in_vmem, (within, high, low, prior, gates)), in_hbm(matrix), in_vmem(resid), in_hbm(select))


def add_part(total, part_ref, matrix_ref, shift):
    inner = part_ref.shape[1]
    parts = matrix_ref.shape[0] // inner
    source = (lax.axis_index("tp") + parts - shift) % parts
    return total + dot_nn(part_ref[...], matrix_ref[pl.ds(source * inner, inner), :])


def more_kernel(part_ref, matrix_ref, total_ref, out_ref, *, shift):
    out_ref[...] = add_part(total_ref[...], part_ref, matrix_ref, shift)


def project_more(part, shift, matrix, total):
    here = pl.BlockSpec(memory_space=pltpu.VMEM)
    return pl.pallas_call(
        functools.partial(more_kernel, shift=shift),
        in_specs=[here, here, here],
        out_specs=here,
        out_shape=pltpu.VMEM(total.shape, F32),
        compiler_params=params(16),
        name="project_more",
    )(*map(in_vmem, (part, matrix, total)))


def project_kernel(part_ref, matrix_ref, total_ref, scale_ref, select_ref, stream_ref, packed_ref, stream_out, stacked, sem, *, shift):
    stream = add_part(total_ref[...], part_ref, matrix_ref, shift).astype(BF16)
    stream_out[...] = stream
    stream_copy = pltpu.make_async_copy(stream_out, stream_ref, sem)
    stream_copy.start()
    values = stream.astype(F32)
    square = jnp.mean(values * values, axis=1, keepdims=True)
    normed = (values * lax.rsqrt(square + 1e-06) * scale_ref[...]).astype(BF16)
    rows = normed.shape[0]
    half = normed.shape[1] // 2
    stacked[0:rows, :] = normed[:, :half]
    stacked[rows : 2 * rows, :] = normed[:, half:]
    packed_ref[...] = dot_nn(select_ref[...], stacked[...]).astype(BF16)
    stream_copy.wait()


def project(part, shift, matrix, total, scale, select):
    rows, width = total.shape
    slots = select.shape[0]
    here = pl.BlockSpec(memory_space=pltpu.VMEM)
    return pl.pallas_call(
        functools.partial(project_kernel, shift=shift),
        in_specs=[here, here, here, pl.BlockSpec((1, width), lambda: (0, 0)), here],
        out_specs=[pl.BlockSpec(memory_space=pl.ANY), here],
        scratch_shapes=[
            pltpu.VMEM((rows, width), BF16),
            pltpu.VMEM((2 * rows, width // 2), BF16),
            pltpu.SemaphoreType.DMA,
        ],
        out_shape=[pltpu.HBM((rows, width), BF16), pltpu.VMEM((slots, width // 2), BF16)],
        compiler_params=params(24),
        name="project",
    )(in_vmem(part), in_vmem(matrix), in_vmem(total), in_hbm(scale), in_vmem(select))


def expert_kernel(slots_ref, gate_ref, up_ref, down_ref, out_ref, rows_in, hidden, outs, sems):
    half = slots_ref.shape[1]
    split, rows2, wide = outs.shape
    rows = rows2 // 2
    cols = [slice(i * wide, (i + 1) * wide) for i in range(split)]
    out_copies = [pltpu.make_async_copy(outs.at[i], out_ref.at[:, cols[i]], sems.at[i]) for i in range(split)]
    group = 64
    upper = lax.broadcasted_iota(jnp.int32, (group // 16, 8, half), 1) < 4

    def untangle(i, carry):
        block = slots_ref[pl.ds(i * group, group), :].astype(F32).reshape(group // 16, 2, 8, half)
        one, two = (block[:, 0], block[:, 1])
        low = jnp.where(upper, one, pltpu.roll(two, 4, 1))
        high = jnp.where(upper, pltpu.roll(one, 4, 1), two)
        at = pl.ds(i * (group // 2), group // 2)
        rows_in[at, 0:half] = low.reshape(group // 2, half).astype(BF16)
        rows_in[at, half : 2 * half] = high.reshape(group // 2, half).astype(BF16)
        return carry

    lax.fori_loop(0, slots_ref.shape[0] // group, untangle, 0)

    for i in range(split):
        gates = dot_nn(rows_in[...], gate_ref[0, :, cols[i]])
        ups = dot_nn(rows_in[...], up_ref[0, :, cols[i]])
        hidden[:, cols[i]] = (gates / (1.0 + jnp.exp(-gates)) * ups).astype(BF16)

    top = lax.broadcasted_iota(jnp.int32, (rows // 8, 8, wide), 1) < 4
    for i in range(split):
        low = dot_nn(hidden[...], down_ref[0, :, cols[i]]).reshape(-1, 8, wide)
        high = dot_nn(hidden[...], down_ref[0, :, half + i * wide : half + (i + 1) * wide]).reshape(-1, 8, wide)
        one = jnp.where(top, low, pltpu.roll(high, 4, 1))
        two = jnp.where(top, pltpu.roll(low, 4, 1), high)
        outs[i] = jnp.stack([one, two], axis=1).reshape(2 * rows, wide).astype(BF16)
        out_copies[i].start()
    for i in range(split):
        out_copies[i].wait()


def experts_on(slots, gate_matrix, up_matrix, down_matrix):
    rows, half = slots.shape
    width, inner = gate_matrix.shape[1:]
    split = 4
    here = pl.BlockSpec(memory_space=pltpu.VMEM)
    return pl.pallas_call(
        expert_kernel,
        in_specs=[here, here, here, here],
        out_specs=pl.BlockSpec(memory_space=pl.ANY),
        out_shape=pltpu.HBM((rows, half), BF16),
        scratch_shapes=[
            pltpu.VMEM((rows // 2, width), BF16),
            pltpu.VMEM((rows // 2, inner), BF16),
            pltpu.VMEM((split, rows, half // split), BF16),
            pltpu.SemaphoreType.DMA((split,)),
        ],
        compiler_params=params(24),
        name="experts_on",
    )(*map(in_vmem, (slots, gate_matrix, up_matrix, down_matrix)))


def combine_kernel(returned_ref, pick_ref, weight_ref, stream_ref, out_ref, stream_in, outs, sems):
    rows, _ = stream_in.shape
    half = returned_ref.shape[1]
    stream_copy = pltpu.make_async_copy(stream_ref, stream_in, sems.at[0])
    stream_copy.start()
    weights = weight_ref[...]
    wide = outs.shape[2]
    copies = []
    for n in range(half // wide):
        picked = dot_nn(pick_ref[...], returned_ref[:, n * wide : (n + 1) * wide])
        if n == 0:
            stream_copy.wait()
        for j in range(2):
            at = 2 * j * rows
            cols = slice(j * half + n * wide, j * half + (n + 1) * wide)
            added = weights[:, 0:1] * picked[at : at + rows] + weights[:, 1:2] * picked[at + rows : at + 2 * rows]
            slot = 2 * n + j
            outs[slot] = (stream_in[:, cols].astype(F32) + added).astype(BF16)
            copies.append(pltpu.make_async_copy(outs.at[slot], out_ref.at[:, cols], sems.at[slot + 1]))
            copies[-1].start()
    for copy in copies:
        copy.wait()


def combine(returned, pick, stream, routing_weight):
    rows, width = stream.shape
    here = pl.BlockSpec(memory_space=pltpu.VMEM)
    there = pl.BlockSpec(memory_space=pl.ANY)
    pieces = 4
    return pl.pallas_call(
        combine_kernel,
        in_specs=[here, here, here, there],
        out_specs=there,
        out_shape=pltpu.HBM(stream.shape, BF16),
        scratch_shapes=[
            pltpu.VMEM((rows, width), BF16),
            pltpu.VMEM((pieces, rows, width // pieces), BF16),
            pltpu.SemaphoreType.DMA((pieces + 1,)),
        ],
        compiler_params=params(24),
        name="combine",
    )(in_vmem(returned), in_vmem(pick), in_vmem(routing_weight), in_hbm(stream))


def body(
    resid,
    query,
    forget_logits,
    forget_margin,
    decay_spike,
    value_logits,
    output_gate_logits,
    head_norm_scale,
    output_matrix,
    norm_scale_vector,
    routes,
    routing_weight,
    gate_matrix,
    up_matrix,
    down_matrix,
):
    rows, top = routes.shape
    experts = lax.axis_size(SP) * lax.axis_size("tp")
    capacity = 2 * rows * top // experts
    width = resid.shape[1]
    margin = forget_margin[None, :]
    places = lax.axis_size("tp")
    cum, values, start, sent = local_states(forget_logits, value_logits, margin, decay_spike.T)
    select, pick = slots_of(routes, experts, capacity)
    parts = lax.all_to_all(sent, SP, split_axis=0, concat_axis=0, tiled=True)
    within, high, low, gates = within_blocks(
        query, forget_logits, margin, cum, values, start, output_gate_logits, head_norm_scale[None, :]
    )
    prior = lax.all_to_all(carried_in(parts), SP, split_axis=0, concat_axis=0, tiled=True)
    prior = prior.reshape(start.shape[1], DK)
    shifts = (2, 1, places - 1)
    arrived = []
    for k in shifts:
        gated = gated_rows(k, within, high, low, prior, gates)
        arrived.append(lax.ppermute(gated, "tp", [(i, (i + k) % places) for i in range(places)]))
    total, matrix, select = project_own(within, high, low, prior, gates, output_matrix, resid, select)
    total = project_more(arrived[0], shifts[0], matrix, total)
    total = project_more(arrived[1], shifts[1], matrix, total)
    stream, packed = project(arrived[2], shifts[2], matrix, total, norm_scale_vector[None, :], select)
    shape = (experts, 2 * capacity, width // 2)
    slots = lax.all_to_all(packed.reshape(shape), SP_TP, split_axis=0, concat_axis=0, tiled=True)
    answers = experts_on(slots.reshape(packed.shape), gate_matrix, up_matrix, down_matrix)
    returned = lax.all_to_all(answers.reshape(shape), SP_TP, split_axis=0, concat_axis=0, tiled=True)
    return combine(returned.reshape(packed.shape), pick, stream, routing_weight)


def solution(mesh):
    finer = Mesh(mesh.devices.reshape(4, 4, 2, mesh.shape["tp"]), SP_TP)
    placed = (
        P(SP_TP, None),
        P(SP, "tp"),
        P(SP, "tp"),
        P("tp"),
        P(SP, "tp"),
        P(SP, "tp"),
        P(SP, "tp"),
        P("tp"),
        P(),
        P(),
        P(SP_TP, None),
        P(SP_TP, None),
        P(SP_TP, None, None),
        P(SP_TP, None, None),
        P(SP_TP, None, None),
    )
    return jax.shard_map(
        body, mesh=finer, in_specs=placed, out_specs=P(SP_TP, None), check_vma=False
    )
```

```python
import functools

import jax
import jax.numpy as jnp
from jax import lax
from jax.experimental import pallas as pl
from jax.experimental.pallas import tpu as pltpu
from jax.sharding import Mesh
from jax.sharding import PartitionSpec as P

DK = 128
CHUNK = 128
SP = ("sp_0", "sp_1", "sp_2")
SP_TP = ("sp_0", "sp_1", "sp_2", "tp")
F32 = jnp.float32
BF16 = jnp.bfloat16


def dot_nn(a, b):
    return lax.dot_general(a, b, (((1,), (0,)), ((), ())), preferred_element_type=F32)


def dot_nt(a, b):
    return lax.dot_general(a, b, (((1,), (1,)), ((), ())), preferred_element_type=F32)


def dot_tn(a, b):
    return lax.dot_general(a, b, (((0,), (0,)), ((), ())), preferred_element_type=F32)


def lower_mask(n, strict):
    row = lax.broadcasted_iota(jnp.int32, (n, n), 0)
    col = lax.broadcasted_iota(jnp.int32, (n, n), 1)
    return row > col if strict else row >= col


def in_hbm(value):
    return pltpu.with_memory_space_constraint(value, pltpu.HBM)


def in_vmem(value):
    return pltpu.with_memory_space_constraint(value, pltpu.VMEM)


def params(mebibytes):
    return pltpu.CompilerParams(vmem_limit_bytes=mebibytes * 1024 * 1024)


def sigmoid(value):
    return 1.0 / (1.0 + jnp.exp(-value))


def halves(value):
    high = value.astype(BF16)
    return high, (value - high.astype(F32)).astype(BF16)


def state_kernel(forget_ref, value_ref, margin_ref, spike_ref, cum_ref, values_ref, start_ref, sent_ref, state, before, keys_in, decays):
    step = pl.program_id(0)
    heads = forget_ref.shape[1] // DK

    @pl.when(step == 0)
    def _():
        state[...] = jnp.zeros_like(state)
        before[...] = jnp.zeros_like(before)

    tri = lower_mask(CHUNK, False).astype(BF16)
    tri = jnp.concatenate([tri, tri], axis=1)
    blocks = [slice(c * CHUNK, (c + 1) * CHUNK) for c in range(forget_ref.shape[0] // CHUNK)]
    for c, rows in enumerate(blocks):
        for h in range(heads):
            cols = slice(h * DK, (h + 1) * DK)
            keys = margin_ref[:, cols] * sigmoid(-forget_ref[rows, cols].astype(F32))
            keys_in[rows, cols] = keys
            decays[c, 0:CHUNK, cols], decays[c, CHUNK : 2 * CHUNK, cols] = halves(jnp.log(1.0 - keys))
    for c, rows in enumerate(blocks):
        spikes = dot_nt(tri, jnp.concatenate(halves(spike_ref[:, rows]), axis=1))
        sums = dot_nn(tri, decays[c])
        for h in range(heads):
            cols = slice(h * DK, (h + 1) * DK)
            cum_ref[rows, cols] = sums[:, cols] + spikes[:, h : h + 1]
    for c, rows in enumerate(blocks):
        start_ref[c] = state[...]
        for h in range(heads):
            cols = slice(h * DK, (h + 1) * DK)
            cum = cum_ref[rows, cols]
            last = cum[CHUNK - 1 : CHUNK, :]
            logits = value_ref[rows, cols].astype(F32)
            values = (logits * sigmoid(logits)).astype(BF16)
            values_ref[rows, cols] = values
            kept = (keys_in[rows, cols] * jnp.exp(last - cum)).astype(BF16)
            state[cols, :] = jnp.exp(last) * state[cols, :] + dot_tn(values, kept)
            before[:, cols] = before[:, cols] + last

    @pl.when(step == pl.num_programs(0) - 1)
    def _():
        share = DK // 8
        first = lax.broadcasted_iota(jnp.int32, (TAIL, DK), 0) == 0
        for h in range(heads):
            total = before[:, h * DK : (h + 1) * DK]
            high = total.astype(BF16).astype(F32)
            tail = jnp.where(first, high, total - high).astype(BF16)
            for i in range(8):
                row = h * DK + i * share
                sent_ref[h * 8 + i, 0:share, :] = state[row : row + share, :].astype(BF16)
                sent_ref[h * 8 + i, share : share + TAIL, :] = tail


STATE_STEPS = 2
TAIL = 8


def local_states(forget_logits, value_logits, margin, spike):
    rows, width = forget_logits.shape
    heads = width // DK
    size = rows // STATE_STEPS
    by_rows = lambda i: (i, 0)
    return pl.pallas_call(
        state_kernel,
        grid=(STATE_STEPS,),
        in_specs=[
            pl.BlockSpec((size, width), by_rows),
            pl.BlockSpec((size, width), by_rows),
            pl.BlockSpec((1, width), lambda i: (0, 0)),
            pl.BlockSpec((heads, size), lambda i: (0, i)),
        ],
        out_specs=[
            pl.BlockSpec((size, width), by_rows),
            pl.BlockSpec((size, width), by_rows),
            pl.BlockSpec((size // CHUNK, width, DK), lambda i: (i, 0, 0)),
            pl.BlockSpec((heads * 8, DK // 8 + TAIL, DK), lambda i: (0, 0, 0)),
        ],
        out_shape=[
            pltpu.HBM((rows, width), F32),
            pltpu.HBM((rows, width), BF16),
            pltpu.HBM((rows // CHUNK, width, DK), F32),
            pltpu.HBM((heads * 8, DK // 8 + TAIL, DK), BF16),
        ],
        scratch_shapes=[
            pltpu.VMEM((width, DK), F32),
            pltpu.VMEM((1, width), F32),
            pltpu.VMEM((size, width), F32),
            pltpu.VMEM((size // CHUNK, 2 * CHUNK, width), BF16),
        ],
        compiler_params=params(16),
        name="local_states",
    )(*map(in_hbm, (forget_logits, value_logits, margin, spike)))


def carry_kernel(parts_ref, prior_ref):
    share = prior_ref.shape[1]
    running = jnp.zeros(prior_ref.shape[1:], F32)
    for d in range(parts_ref.shape[0]):
        prior_ref[d] = running
        tail = parts_ref[d, share : share + TAIL, :].astype(F32)
        total = tail[0:1, :] + tail[1:2, :]
        running = jnp.exp(total) * running + parts_ref[d, 0:share, :].astype(F32)


def carried_in(parts):
    return pl.pallas_call(
        carry_kernel,
        out_shape=pltpu.HBM((parts.shape[0], parts.shape[1] - TAIL, parts.shape[2]), F32),
        compiler_params=params(8),
        name="carried_in",
    )(parts)


def dot_split(queries, states):
    return dot_nt(queries[0], states[0]) + dot_nt(queries[0], states[1]) + dot_nt(queries[1], states[0])


def within_kernel(query_ref, forget_ref, margin_ref, cum_ref, values_ref, start_ref, gate_ref, scale_ref, out_ref, high_ref, low_ref, gates_ref, before):
    heads = query_ref.shape[1] // DK
    causal = lower_mask(CHUNK, False)

    @pl.when(pl.program_id(0) == 0)
    def _():
        before[...] = jnp.zeros_like(before)

    for h in range(heads):
        cols = slice(h * DK, (h + 1) * DK)
        cum = cum_ref[:, cols]
        spread = cum - cum[CHUNK // 2 - 1 : CHUNK // 2, :]
        keys = margin_ref[:, cols] * sigmoid(-forget_ref[:, cols].astype(F32))
        queries = query_ref[:, cols].astype(F32) * (DK**-0.5)
        scores = dot_nt((queries * jnp.exp(spread)).astype(BF16), (keys * jnp.exp(-spread)).astype(BF16))
        scores = jnp.where(causal, scores, 0.0).astype(BF16)
        decayed = queries * jnp.exp(cum)
        earlier = dot_split(halves(decayed), halves(start_ref[0, cols, :]))
        out_ref[:, cols] = dot_nn(scores, values_ref[:, cols]) + earlier
        high_ref[:, cols], low_ref[:, cols] = halves(decayed * jnp.exp(before[:, cols]))
        before[:, cols] = before[:, cols] + cum[CHUNK - 1 : CHUNK, :]
        logits = gate_ref[:, cols].astype(F32)
        gates_ref[:, cols] = scale_ref[:, cols] * (logits * sigmoid(logits))


def within_blocks(query, forget_logits, margin, cum, values, start, gate_logits, scale):
    rows, width = query.shape
    block = pl.BlockSpec((CHUNK, width), lambda i: (i, 0))
    row = pl.BlockSpec((1, width), lambda i: (0, 0))
    return pl.pallas_call(
        within_kernel,
        grid=(rows // CHUNK,),
        in_specs=[block, block, row, block, block, pl.BlockSpec((1, width, DK), lambda i: (i, 0, 0)), block, row],
        out_specs=[block, block, block, block],
        out_shape=[pltpu.VMEM((rows, width), kind) for kind in (F32, BF16, BF16, F32)],
        scratch_shapes=[pltpu.VMEM((1, width), F32)],
        compiler_params=params(24),
        name="within_blocks",
    )(*map(in_hbm, (query, forget_logits, margin, cum, values, start, gate_logits, scale)))


def readout(within_ref, high_ref, low_ref, prior_ref, gates_ref, out_ref, shift):
    heads = within_ref.shape[1] // DK
    blocks = within_ref.shape[0] // CHUNK
    rows = pl.ds((lax.axis_index("tp") + shift) % blocks * CHUNK, CHUNK)
    for h in range(heads):
        cols = slice(h * DK, (h + 1) * DK)
        carried = dot_split((high_ref[rows, cols], low_ref[rows, cols]), halves(prior_ref[cols, :]))
        recurrent = within_ref[rows, cols] + carried
        square = jnp.mean(recurrent * recurrent, axis=1, keepdims=True)
        out_ref[:, cols] = (recurrent * lax.rsqrt(square + 1e-06) * gates_ref[rows, cols]).astype(BF16)


def readout_kernel(*refs, shift):
    readout(*refs, shift)


def gated_rows(shift, within, high, low, prior, gates):
    here = pl.BlockSpec(memory_space=pltpu.VMEM)
    return pl.pallas_call(
        functools.partial(readout_kernel, shift=shift),
        in_specs=[here] * 5,
        out_specs=here,
        out_shape=pltpu.VMEM((CHUNK, within.shape[1]), BF16),
        compiler_params=params(16),
        name="gated_rows",
    )(*map(in_vmem, (within, high, low, prior, gates)))


def slot_positions(routes, experts, capacity):
    rows = routes.shape[0]
    lanes = lax.broadcasted_iota(jnp.int32, (rows, experts), 1)
    first, second = (routes[:, 0:1], routes[:, 1:2])
    one, two = (lanes == first, lanes == second)
    named = (one.astype(F32) + two.astype(F32)).astype(BF16)
    earlier = dot_nn(lower_mask(rows, True).astype(BF16), named)
    ranks = [
        jnp.sum(jnp.where(hit, earlier, 0.0), axis=1, keepdims=True).astype(jnp.int32)
        for hit in (one, two)
    ]
    return [expert * (2 * capacity) + rank for expert, rank in zip((first, second), ranks)]


def slots_kernel(routes_ref, select_ref, pick_ref, *, experts, capacity):
    rows = routes_ref.shape[0]
    slots = 2 * experts * capacity
    places = slot_positions(routes_ref[...], experts, capacity)
    lanes = lax.broadcasted_iota(jnp.int32, (rows, slots), 1)
    down = lax.broadcasted_iota(jnp.int32, (slots, rows), 0)
    across = [
        jnp.transpose(jnp.broadcast_to(place.astype(F32), (rows, rows)))[0:1, :].astype(jnp.int32)
        for place in places
    ]
    for j in range(2):
        hit = (down == across[0] + j * capacity) | (down == across[1] + j * capacity)
        select_ref[:, j * rows : (j + 1) * rows] = jnp.where(hit, 1.0, 0.0).astype(BF16)
        for k in range(2):
            at = (2 * j + k) * rows
            pick_ref[at : at + rows, :] = jnp.where(lanes == places[k] + j * capacity, 1.0, 0.0).astype(BF16)


def slots_of(routes, experts, capacity):
    rows = routes.shape[0]
    slots = 2 * experts * capacity
    return pl.pallas_call(
        functools.partial(slots_kernel, experts=experts, capacity=capacity),
        out_shape=[pltpu.HBM((slots, 2 * rows), BF16), pltpu.HBM((4 * rows, slots), BF16)],
        compiler_params=params(12),
        name="slots_of",
    )(routes)


def own_kernel(within_ref, high_ref, low_ref, prior_ref, gates_ref, matrix_ref, resid_ref, select_ref, total_ref, matrix_out_ref, select_out_ref, own, sems):
    place = lax.axis_index("tp")
    inner = own.shape[1]
    parts = sems.shape[0] - 1
    copies = []
    for k in range(parts):
        at = pl.ds((place + k) % parts * inner, inner)
        copies.append(pltpu.make_async_copy(matrix_ref.at[at, :], matrix_out_ref.at[at, :], sems.at[k]))
    copies.append(pltpu.make_async_copy(select_ref, select_out_ref, sems.at[parts]))
    for copy in copies:
        copy.start()
    readout(within_ref, high_ref, low_ref, prior_ref, gates_ref, own, 0)
    copies[0].wait()
    part = dot_nn(own[...], matrix_out_ref[pl.ds(place * inner, inner), :])
    total_ref[...] = resid_ref[...].astype(F32) + part
    for copy in copies[1:]:
        copy.wait()


def project_own(within, high, low, prior, gates, matrix, resid, select):
    here = pl.BlockSpec(memory_space=pltpu.VMEM)
    there = pl.BlockSpec(memory_space=pl.ANY)
    inner = within.shape[1]
    return pl.pallas_call(
        own_kernel,
        in_specs=[here, here, here, here, here, there, here, there],
        out_specs=[here, here, here],
        out_shape=[
            pltpu.VMEM(resid.shape, F32),
            pltpu.VMEM(matrix.shape, BF16),
            pltpu.VMEM(select.shape, BF16),
        ],
        scratch_shapes=[
            pltpu.VMEM((CHUNK, inner), BF16),
            pltpu.SemaphoreType.DMA((matrix.shape[0] // inner + 1,)),
        ],
        compiler_params=params(16),
        name="project_own",
    )(*map(in_vmem, (within, high, low, prior, gates)), in_hbm(matrix), in_vmem(resid), in_hbm(select))


def add_part(total, part_ref, matrix_ref, shift):
    inner = part_ref.shape[1]
    parts = matrix_ref.shape[0] // inner
    source = (lax.axis_index("tp") + parts - shift) % parts
    return total + dot_nn(part_ref[...], matrix_ref[pl.ds(source * inner, inner), :])


def more_kernel(part_ref, matrix_ref, total_ref, out_ref, *, shift):
    out_ref[...] = add_part(total_ref[...], part_ref, matrix_ref, shift)


def project_more(part, shift, matrix, total):
    here = pl.BlockSpec(memory_space=pltpu.VMEM)
    return pl.pallas_call(
        functools.partial(more_kernel, shift=shift),
        in_specs=[here, here, here],
        out_specs=here,
        out_shape=pltpu.VMEM(total.shape, F32),
        compiler_params=params(16),
        name="project_more",
    )(*map(in_vmem, (part, matrix, total)))


def project_kernel(part_ref, matrix_ref, total_ref, scale_ref, select_ref, stream_ref, packed_ref, stream_out, stacked, sem, *, shift):
    stream = add_part(total_ref[...], part_ref, matrix_ref, shift).astype(BF16)
    stream_out[...] = stream
    stream_copy = pltpu.make_async_copy(stream_out, stream_ref, sem)
    stream_copy.start()
    values = stream.astype(F32)
    square = jnp.mean(values * values, axis=1, keepdims=True)
    normed = (values * lax.rsqrt(square + 1e-06) * scale_ref[...]).astype(BF16)
    rows = normed.shape[0]
    half = normed.shape[1] // 2
    stacked[0:rows, :] = normed[:, :half]
    stacked[rows : 2 * rows, :] = normed[:, half:]
    packed_ref[...] = dot_nn(select_ref[...], stacked[...]).astype(BF16)
    stream_copy.wait()


def project(part, shift, matrix, total, scale, select):
    rows, width = total.shape
    slots = select.shape[0]
    here = pl.BlockSpec(memory_space=pltpu.VMEM)
    return pl.pallas_call(
        functools.partial(project_kernel, shift=shift),
        in_specs=[here, here, here, here, here],
        out_specs=[pl.BlockSpec(memory_space=pl.ANY), here],
        scratch_shapes=[
            pltpu.VMEM((rows, width), BF16),
            pltpu.VMEM((2 * rows, width // 2), BF16),
            pltpu.SemaphoreType.DMA,
        ],
        out_shape=[pltpu.HBM((rows, width), BF16), pltpu.VMEM((slots, width // 2), BF16)],
        compiler_params=params(24),
        name="project",
    )(*map(in_vmem, (part, matrix, total, scale, select)))


def expert_kernel(slots_ref, gate_ref, up_ref, down_ref, out_ref, rows_in, hidden, outs, sems):
    half = slots_ref.shape[1]
    split, rows2, wide = outs.shape
    rows = rows2 // 2
    cols = [slice(i * wide, (i + 1) * wide) for i in range(split)]
    out_copies = [pltpu.make_async_copy(outs.at[i], out_ref.at[:, cols[i]], sems.at[i]) for i in range(split)]
    group = 64
    upper = lax.broadcasted_iota(jnp.int32, (group // 16, 8, half), 1) < 4

    for i in range(slots_ref.shape[0] // group):
        block = slots_ref[i * group : (i + 1) * group, :].astype(F32).reshape(group // 16, 2, 8, half)
        one, two = (block[:, 0], block[:, 1])
        low = jnp.where(upper, one, pltpu.roll(two, 4, 1))
        high = jnp.where(upper, pltpu.roll(one, 4, 1), two)
        at = slice(i * (group // 2), (i + 1) * (group // 2))
        rows_in[at, 0:half] = low.reshape(group // 2, half).astype(BF16)
        rows_in[at, half : 2 * half] = high.reshape(group // 2, half).astype(BF16)

    for i in range(split):
        gates = dot_nn(rows_in[...], gate_ref[0, :, cols[i]])
        ups = dot_nn(rows_in[...], up_ref[0, :, cols[i]])
        hidden[:, cols[i]] = (gates / (1.0 + jnp.exp(-gates)) * ups).astype(BF16)

    top = lax.broadcasted_iota(jnp.int32, (rows // 8, 8, wide), 1) < 4
    for i in range(split):
        low = dot_nn(hidden[...], down_ref[0, :, cols[i]]).reshape(-1, 8, wide)
        high = dot_nn(hidden[...], down_ref[0, :, half + i * wide : half + (i + 1) * wide]).reshape(-1, 8, wide)
        one = jnp.where(top, low, pltpu.roll(high, 4, 1))
        two = jnp.where(top, pltpu.roll(low, 4, 1), high)
        outs[i] = jnp.stack([one, two], axis=1).reshape(2 * rows, wide).astype(BF16)
        out_copies[i].start()
    for i in range(split):
        out_copies[i].wait()


def experts_on(slots, gate_matrix, up_matrix, down_matrix):
    rows, half = slots.shape
    width, inner = gate_matrix.shape[1:]
    split = 4
    here = pl.BlockSpec(memory_space=pltpu.VMEM)
    return pl.pallas_call(
        expert_kernel,
        in_specs=[here, here, here, here],
        out_specs=pl.BlockSpec(memory_space=pl.ANY),
        out_shape=pltpu.HBM((rows, half), BF16),
        scratch_shapes=[
            pltpu.VMEM((rows // 2, width), BF16),
            pltpu.VMEM((rows // 2, inner), BF16),
            pltpu.VMEM((split, rows, half // split), BF16),
            pltpu.SemaphoreType.DMA((split,)),
        ],
        compiler_params=params(24),
        name="experts_on",
    )(*map(in_vmem, (slots, gate_matrix, up_matrix, down_matrix)))


def combine_kernel(returned_ref, pick_ref, weight_ref, stream_ref, out_ref, stream_in, outs, sems):
    rows, _ = stream_in.shape
    half = returned_ref.shape[1]
    stream_copy = pltpu.make_async_copy(stream_ref, stream_in, sems.at[0])
    stream_copy.start()
    weights = weight_ref[...]
    wide = outs.shape[2]
    copies = []
    for n in range(half // wide):
        picked = dot_nn(pick_ref[...], returned_ref[:, n * wide : (n + 1) * wide])
        if n == 0:
            stream_copy.wait()
        for j in range(2):
            at = 2 * j * rows
            cols = slice(j * half + n * wide, j * half + (n + 1) * wide)
            added = weights[:, 0:1] * picked[at : at + rows] + weights[:, 1:2] * picked[at + rows : at + 2 * rows]
            slot = 2 * n + j
            outs[slot] = (stream_in[:, cols].astype(F32) + added).astype(BF16)
            copies.append(pltpu.make_async_copy(outs.at[slot], out_ref.at[:, cols], sems.at[slot + 1]))
            copies[-1].start()
    for copy in copies:
        copy.wait()


def combine(returned, pick, stream, routing_weight):
    rows, width = stream.shape
    here = pl.BlockSpec(memory_space=pltpu.VMEM)
    there = pl.BlockSpec(memory_space=pl.ANY)
    pieces = 4
    return pl.pallas_call(
        combine_kernel,
        in_specs=[here, here, here, there],
        out_specs=there,
        out_shape=pltpu.HBM(stream.shape, BF16),
        scratch_shapes=[
            pltpu.VMEM((rows, width), BF16),
            pltpu.VMEM((pieces, rows, width // pieces), BF16),
            pltpu.SemaphoreType.DMA((pieces + 1,)),
        ],
        compiler_params=params(24),
        name="combine",
    )(in_vmem(returned), in_vmem(pick), in_vmem(routing_weight), in_hbm(stream))


def body(
    resid,
    query,
    forget_logits,
    forget_margin,
    decay_spike,
    value_logits,
    output_gate_logits,
    head_norm_scale,
    output_matrix,
    norm_scale_vector,
    routes,
    routing_weight,
    gate_matrix,
    up_matrix,
    down_matrix,
):
    rows, top = routes.shape
    experts = lax.axis_size(SP) * lax.axis_size("tp")
    capacity = 2 * rows * top // experts
    width = resid.shape[1]
    margin = forget_margin[None, :]
    places = lax.axis_size("tp")
    cum, values, start, sent = local_states(forget_logits, value_logits, margin, decay_spike.T)
    select, pick = slots_of(routes, experts, capacity)
    parts = lax.all_to_all(sent, SP, split_axis=0, concat_axis=0, tiled=True)
    within, high, low, gates = within_blocks(
        query, forget_logits, margin, cum, values, start, output_gate_logits, head_norm_scale[None, :]
    )
    prior = lax.all_to_all(carried_in(parts), SP, split_axis=0, concat_axis=0, tiled=True)
    prior = prior.reshape(start.shape[1], DK)
    shifts = (2, 1, places - 1)
    arrived = []
    for k in shifts:
        gated = gated_rows(k, within, high, low, prior, gates)
        arrived.append(lax.ppermute(gated, "tp", [(i, (i + k) % places) for i in range(places)]))
    total, matrix, select = project_own(within, high, low, prior, gates, output_matrix, resid, select)
    total = project_more(arrived[0], shifts[0], matrix, total)
    total = project_more(arrived[1], shifts[1], matrix, total)
    stream, packed = project(arrived[2], shifts[2], matrix, total, norm_scale_vector[None, :], select)
    shape = (experts, 2 * capacity, width // 2)
    slots = lax.all_to_all(packed.reshape(shape), SP_TP, split_axis=0, concat_axis=0, tiled=True)
    answers = experts_on(slots.reshape(packed.shape), gate_matrix, up_matrix, down_matrix)
    returned = lax.all_to_all(answers.reshape(shape), SP_TP, split_axis=0, concat_axis=0, tiled=True)
    return combine(returned.reshape(packed.shape), pick, stream, routing_weight)


def solution(mesh):
    finer = Mesh(mesh.devices.reshape(4, 4, 2, mesh.shape["tp"]), SP_TP)
    placed = (
        P(SP_TP, None),
        P(SP, "tp"),
        P(SP, "tp"),
        P("tp"),
        P(SP, "tp"),
        P(SP, "tp"),
        P(SP, "tp"),
        P("tp"),
        P(),
        P(),
        P(SP_TP, None),
        P(SP_TP, None),
        P(SP_TP, None, None),
        P(SP_TP, None, None),
        P(SP_TP, None, None),
    )
    return jax.shard_map(
        body, mesh=finer, in_specs=placed, out_specs=P(SP_TP, None), check_vma=False
    )
```

```python
import functools

import jax
import jax.numpy as jnp
from jax import lax
from jax.experimental import pallas as pl
from jax.experimental.pallas import tpu as pltpu
from jax.sharding import Mesh
from jax.sharding import PartitionSpec as P

DK = 128
CHUNK = 128
SP = ("sp_0", "sp_1", "sp_2")
SP_TP = ("sp_0", "sp_1", "sp_2", "tp")
F32 = jnp.float32
BF16 = jnp.bfloat16


def dot_nn(a, b):
    return lax.dot_general(a, b, (((1,), (0,)), ((), ())), preferred_element_type=F32)


def dot_nt(a, b):
    return lax.dot_general(a, b, (((1,), (1,)), ((), ())), preferred_element_type=F32)


def dot_tn(a, b):
    return lax.dot_general(a, b, (((0,), (0,)), ((), ())), preferred_element_type=F32)


def lower_mask(n, strict):
    row = lax.broadcasted_iota(jnp.int32, (n, n), 0)
    col = lax.broadcasted_iota(jnp.int32, (n, n), 1)
    return row > col if strict else row >= col


def in_hbm(value):
    return pltpu.with_memory_space_constraint(value, pltpu.HBM)


def in_vmem(value):
    return pltpu.with_memory_space_constraint(value, pltpu.VMEM)


def params(mebibytes):
    return pltpu.CompilerParams(vmem_limit_bytes=mebibytes * 1024 * 1024)


def sigmoid(value):
    return 1.0 / (1.0 + jnp.exp(-value))


def halves(value):
    high = value.astype(BF16)
    return high, (value - high.astype(F32)).astype(BF16)


def state_kernel(forget_ref, value_ref, margin_ref, spike_ref, cum_ref, start_ref, sent_ref, state, before, keys_in, decays):
    step = pl.program_id(0)
    heads = forget_ref.shape[1] // DK

    @pl.when(step == 0)
    def _():
        state[...] = jnp.zeros_like(state)
        before[...] = jnp.zeros_like(before)

    tri = lower_mask(CHUNK, False).astype(BF16)
    tri = jnp.concatenate([tri, tri], axis=1)
    blocks = [slice(c * CHUNK, (c + 1) * CHUNK) for c in range(forget_ref.shape[0] // CHUNK)]
    for c, rows in enumerate(blocks):
        for h in range(heads):
            cols = slice(h * DK, (h + 1) * DK)
            keys = margin_ref[:, cols] * sigmoid(-forget_ref[rows, cols].astype(F32))
            keys_in[rows, cols] = keys
            decays[c, 0:CHUNK, cols], decays[c, CHUNK : 2 * CHUNK, cols] = halves(jnp.log(1.0 - keys))
    for c, rows in enumerate(blocks):
        spikes = dot_nt(tri, jnp.concatenate(halves(spike_ref[:, rows]), axis=1))
        sums = dot_nn(tri, decays[c])
        for h in range(heads):
            cols = slice(h * DK, (h + 1) * DK)
            cum_ref[rows, cols] = sums[:, cols] + spikes[:, h : h + 1]
    for c, rows in enumerate(blocks):
        start_ref[c] = state[...]
        for h in range(heads):
            cols = slice(h * DK, (h + 1) * DK)
            cum = cum_ref[rows, cols]
            last = cum[CHUNK - 1 : CHUNK, :]
            logits = value_ref[rows, cols].astype(F32)
            values = (logits * sigmoid(logits)).astype(BF16)
            kept = (keys_in[rows, cols] * jnp.exp(last - cum)).astype(BF16)
            state[cols, :] = jnp.exp(last) * state[cols, :] + dot_tn(values, kept)
            before[:, cols] = before[:, cols] + last

    @pl.when(step == pl.num_programs(0) - 1)
    def _():
        share = DK // 8
        first = lax.broadcasted_iota(jnp.int32, (TAIL, DK), 0) == 0
        for h in range(heads):
            total = before[:, h * DK : (h + 1) * DK]
            high = total.astype(BF16).astype(F32)
            tail = jnp.where(first, high, total - high).astype(BF16)
            for i in range(8):
                row = h * DK + i * share
                sent_ref[h * 8 + i, 0:share, :] = state[row : row + share, :].astype(BF16)
                sent_ref[h * 8 + i, share : share + TAIL, :] = tail


STATE_STEPS = 2
TAIL = 8


def local_states(forget_logits, value_logits, margin, spike):
    rows, width = forget_logits.shape
    heads = width // DK
    size = rows // STATE_STEPS
    by_rows = lambda i: (i, 0)
    return pl.pallas_call(
        state_kernel,
        grid=(STATE_STEPS,),
        in_specs=[
            pl.BlockSpec((size, width), by_rows),
            pl.BlockSpec((size, width), by_rows),
            pl.BlockSpec((1, width), lambda i: (0, 0)),
            pl.BlockSpec((heads, size), lambda i: (0, i)),
        ],
        out_specs=[
            pl.BlockSpec((size, width), by_rows),
            pl.BlockSpec((size // CHUNK, width, DK), lambda i: (i, 0, 0)),
            pl.BlockSpec((heads * 8, DK // 8 + TAIL, DK), lambda i: (0, 0, 0)),
        ],
        out_shape=[
            pltpu.HBM((rows, width), F32),
            pltpu.HBM((rows // CHUNK, width, DK), F32),
            pltpu.HBM((heads * 8, DK // 8 + TAIL, DK), BF16),
        ],
        scratch_shapes=[
            pltpu.VMEM((width, DK), F32),
            pltpu.VMEM((1, width), F32),
            pltpu.VMEM((size, width), F32),
            pltpu.VMEM((size // CHUNK, 2 * CHUNK, width), BF16),
        ],
        compiler_params=params(16),
        name="local_states",
    )(*map(in_hbm, (forget_logits, value_logits, margin, spike)))


def carry_kernel(parts_ref, prior_ref):
    share = prior_ref.shape[1]
    running = jnp.zeros(prior_ref.shape[1:], F32)
    for d in range(parts_ref.shape[0]):
        prior_ref[d] = running
        tail = parts_ref[d, share : share + TAIL, :].astype(F32)
        total = tail[0:1, :] + tail[1:2, :]
        running = jnp.exp(total) * running + parts_ref[d, 0:share, :].astype(F32)


def carried_in(parts):
    return pl.pallas_call(
        carry_kernel,
        out_shape=pltpu.HBM((parts.shape[0], parts.shape[1] - TAIL, parts.shape[2]), F32),
        compiler_params=params(8),
        name="carried_in",
    )(parts)


def dot_split(queries, states):
    return dot_nt(queries[0], states[0]) + dot_nt(queries[0], states[1]) + dot_nt(queries[1], states[0])


def within_kernel(query_ref, forget_ref, margin_ref, cum_ref, value_ref, start_ref, gate_ref, scale_ref, out_ref, high_ref, low_ref, gates_ref, before):
    heads = query_ref.shape[1] // DK
    causal = lower_mask(CHUNK, False)

    @pl.when(pl.program_id(0) == 0)
    def _():
        before[...] = jnp.zeros_like(before)

    for h in range(heads):
        cols = slice(h * DK, (h + 1) * DK)
        cum = cum_ref[:, cols]
        spread = cum - cum[CHUNK // 2 - 1 : CHUNK // 2, :]
        keys = margin_ref[:, cols] * sigmoid(-forget_ref[:, cols].astype(F32))
        queries = query_ref[:, cols].astype(F32) * (DK**-0.5)
        scores = dot_nt((queries * jnp.exp(spread)).astype(BF16), (keys * jnp.exp(-spread)).astype(BF16))
        scores = jnp.where(causal, scores, 0.0).astype(BF16)
        decayed = queries * jnp.exp(cum)
        earlier = dot_split(halves(decayed), halves(start_ref[0, cols, :]))
        logits = value_ref[:, cols].astype(F32)
        out_ref[:, cols] = dot_nn(scores, (logits * sigmoid(logits)).astype(BF16)) + earlier
        high_ref[:, cols], low_ref[:, cols] = halves(decayed * jnp.exp(before[:, cols]))
        before[:, cols] = before[:, cols] + cum[CHUNK - 1 : CHUNK, :]
        logits = gate_ref[:, cols].astype(F32)
        gates_ref[:, cols] = scale_ref[:, cols] * (logits * sigmoid(logits))


def within_blocks(query, forget_logits, margin, cum, values, start, gate_logits, scale):
    rows, width = query.shape
    block = pl.BlockSpec((CHUNK, width), lambda i: (i, 0))
    row = pl.BlockSpec((1, width), lambda i: (0, 0))
    return pl.pallas_call(
        within_kernel,
        grid=(rows // CHUNK,),
        in_specs=[block, block, row, block, block, pl.BlockSpec((1, width, DK), lambda i: (i, 0, 0)), block, row],
        out_specs=[block, block, block, block],
        out_shape=[pltpu.VMEM((rows, width), kind) for kind in (F32, BF16, BF16, F32)],
        scratch_shapes=[pltpu.VMEM((1, width), F32)],
        compiler_params=params(24),
        name="within_blocks",
    )(*map(in_hbm, (query, forget_logits, margin, cum, values, start, gate_logits, scale)))


def readout(within_ref, high_ref, low_ref, prior_ref, gates_ref, out_ref, shift):
    heads = within_ref.shape[1] // DK
    blocks = within_ref.shape[0] // CHUNK
    rows = pl.ds((lax.axis_index("tp") + shift) % blocks * CHUNK, CHUNK)
    for h in range(heads):
        cols = slice(h * DK, (h + 1) * DK)
        carried = dot_split((high_ref[rows, cols], low_ref[rows, cols]), halves(prior_ref[cols, :]))
        recurrent = within_ref[rows, cols] + carried
        square = jnp.mean(recurrent * recurrent, axis=1, keepdims=True)
        out_ref[:, cols] = (recurrent * lax.rsqrt(square + 1e-06) * gates_ref[rows, cols]).astype(BF16)


def readout_kernel(*refs, shift):
    readout(*refs, shift)


def gated_rows(shift, within, high, low, prior, gates):
    here = pl.BlockSpec(memory_space=pltpu.VMEM)
    return pl.pallas_call(
        functools.partial(readout_kernel, shift=shift),
        in_specs=[here] * 5,
        out_specs=here,
        out_shape=pltpu.VMEM((CHUNK, within.shape[1]), BF16),
        compiler_params=params(16),
        name="gated_rows",
    )(*map(in_vmem, (within, high, low, prior, gates)))


def slot_positions(routes, experts, capacity):
    rows = routes.shape[0]
    lanes = lax.broadcasted_iota(jnp.int32, (rows, experts), 1)
    first, second = (routes[:, 0:1], routes[:, 1:2])
    one, two = (lanes == first, lanes == second)
    named = (one.astype(F32) + two.astype(F32)).astype(BF16)
    earlier = dot_nn(lower_mask(rows, True).astype(BF16), named)
    ranks = [
        jnp.sum(jnp.where(hit, earlier, 0.0), axis=1, keepdims=True).astype(jnp.int32)
        for hit in (one, two)
    ]
    return [expert * (2 * capacity) + rank for expert, rank in zip((first, second), ranks)]


def slots_kernel(routes_ref, select_ref, pick_ref, *, experts, capacity):
    rows = routes_ref.shape[0]
    slots = 2 * experts * capacity
    places = slot_positions(routes_ref[...], experts, capacity)
    lanes = lax.broadcasted_iota(jnp.int32, (rows, slots), 1)
    down = lax.broadcasted_iota(jnp.int32, (slots, rows), 0)
    across = [
        jnp.transpose(jnp.broadcast_to(place.astype(F32), (rows, rows)))[0:1, :].astype(jnp.int32)
        for place in places
    ]
    for j in range(2):
        hit = (down == across[0] + j * capacity) | (down == across[1] + j * capacity)
        select_ref[:, j * rows : (j + 1) * rows] = jnp.where(hit, 1.0, 0.0).astype(BF16)
        for k in range(2):
            at = (2 * j + k) * rows
            pick_ref[at : at + rows, :] = jnp.where(lanes == places[k] + j * capacity, 1.0, 0.0).astype(BF16)


def slots_of(routes, experts, capacity):
    rows = routes.shape[0]
    slots = 2 * experts * capacity
    return pl.pallas_call(
        functools.partial(slots_kernel, experts=experts, capacity=capacity),
        out_shape=[pltpu.HBM((slots, 2 * rows), BF16), pltpu.HBM((4 * rows, slots), BF16)],
        compiler_params=params(12),
        name="slots_of",
    )(routes)


def own_kernel(within_ref, high_ref, low_ref, prior_ref, gates_ref, matrix_ref, resid_ref, select_ref, total_ref, matrix_out_ref, select_out_ref, own, sems):
    place = lax.axis_index("tp")
    inner = own.shape[1]
    parts = sems.shape[0] - 1
    copies = []
    for k in range(parts):
        at = pl.ds((place + k) % parts * inner, inner)
        copies.append(pltpu.make_async_copy(matrix_ref.at[at, :], matrix_out_ref.at[at, :], sems.at[k]))
    copies.append(pltpu.make_async_copy(select_ref, select_out_ref, sems.at[parts]))
    for copy in copies:
        copy.start()
    readout(within_ref, high_ref, low_ref, prior_ref, gates_ref, own, 0)
    copies[0].wait()
    part = dot_nn(own[...], matrix_out_ref[pl.ds(place * inner, inner), :])
    total_ref[...] = resid_ref[...].astype(F32) + part
    for copy in copies[1:]:
        copy.wait()


def project_own(within, high, low, prior, gates, matrix, resid, select):
    here = pl.BlockSpec(memory_space=pltpu.VMEM)
    there = pl.BlockSpec(memory_space=pl.ANY)
    inner = within.shape[1]
    return pl.pallas_call(
        own_kernel,
        in_specs=[here, here, here, here, here, there, here, there],
        out_specs=[here, here, here],
        out_shape=[
            pltpu.VMEM(resid.shape, F32),
            pltpu.VMEM(matrix.shape, BF16),
            pltpu.VMEM(select.shape, BF16),
        ],
        scratch_shapes=[
            pltpu.VMEM((CHUNK, inner), BF16),
            pltpu.SemaphoreType.DMA((matrix.shape[0] // inner + 1,)),
        ],
        compiler_params=params(16),
        name="project_own",
    )(*map(in_vmem, (within, high, low, prior, gates)), in_hbm(matrix), in_vmem(resid), in_hbm(select))


def add_part(total, part_ref, matrix_ref, shift):
    inner = part_ref.shape[1]
    parts = matrix_ref.shape[0] // inner
    source = (lax.axis_index("tp") + parts - shift) % parts
    return total + dot_nn(part_ref[...], matrix_ref[pl.ds(source * inner, inner), :])


def more_kernel(part_ref, matrix_ref, total_ref, out_ref, *, shift):
    out_ref[...] = add_part(total_ref[...], part_ref, matrix_ref, shift)


def project_more(part, shift, matrix, total):
    here = pl.BlockSpec(memory_space=pltpu.VMEM)
    return pl.pallas_call(
        functools.partial(more_kernel, shift=shift),
        in_specs=[here, here, here],
        out_specs=here,
        out_shape=pltpu.VMEM(total.shape, F32),
        compiler_params=params(16),
        name="project_more",
    )(*map(in_vmem, (part, matrix, total)))


def project_kernel(part_ref, matrix_ref, total_ref, scale_ref, select_ref, stream_ref, packed_ref, stream_out, stacked, sem, *, shift):
    stream = add_part(total_ref[...], part_ref, matrix_ref, shift).astype(BF16)
    stream_out[...] = stream
    stream_copy = pltpu.make_async_copy(stream_out, stream_ref, sem)
    stream_copy.start()
    values = stream.astype(F32)
    square = jnp.mean(values * values, axis=1, keepdims=True)
    normed = (values * lax.rsqrt(square + 1e-06) * scale_ref[...]).astype(BF16)
    rows = normed.shape[0]
    half = normed.shape[1] // 2
    stacked[0:rows, :] = normed[:, :half]
    stacked[rows : 2 * rows, :] = normed[:, half:]
    packed_ref[...] = dot_nn(select_ref[...], stacked[...]).astype(BF16)
    stream_copy.wait()


def project(part, shift, matrix, total, scale, select):
    rows, width = total.shape
    slots = select.shape[0]
    here = pl.BlockSpec(memory_space=pltpu.VMEM)
    return pl.pallas_call(
        functools.partial(project_kernel, shift=shift),
        in_specs=[here, here, here, here, here],
        out_specs=[pl.BlockSpec(memory_space=pl.ANY), here],
        scratch_shapes=[
            pltpu.VMEM((rows, width), BF16),
            pltpu.VMEM((2 * rows, width // 2), BF16),
            pltpu.SemaphoreType.DMA,
        ],
        out_shape=[pltpu.HBM((rows, width), BF16), pltpu.VMEM((slots, width // 2), BF16)],
        compiler_params=params(24),
        name="project",
    )(*map(in_vmem, (part, matrix, total, scale, select)))


def expert_kernel(slots_ref, gate_ref, up_ref, down_ref, out_ref, rows_in, hidden, outs, sems):
    half = slots_ref.shape[1]
    split, rows2, wide = outs.shape
    rows = rows2 // 2
    cols = [slice(i * wide, (i + 1) * wide) for i in range(split)]
    out_copies = [pltpu.make_async_copy(outs.at[i], out_ref.at[:, cols[i]], sems.at[i]) for i in range(split)]
    group = 64
    upper = lax.broadcasted_iota(jnp.int32, (group // 16, 8, half), 1) < 4

    for i in range(slots_ref.shape[0] // group):
        block = slots_ref[i * group : (i + 1) * group, :].astype(F32).reshape(group // 16, 2, 8, half)
        one, two = (block[:, 0], block[:, 1])
        low = jnp.where(upper, one, pltpu.roll(two, 4, 1))
        high = jnp.where(upper, pltpu.roll(one, 4, 1), two)
        at = slice(i * (group // 2), (i + 1) * (group // 2))
        rows_in[at, 0:half] = low.reshape(group // 2, half).astype(BF16)
        rows_in[at, half : 2 * half] = high.reshape(group // 2, half).astype(BF16)

    for i in range(split):
        gates = dot_nn(rows_in[...], gate_ref[0, :, cols[i]])
        ups = dot_nn(rows_in[...], up_ref[0, :, cols[i]])
        hidden[:, cols[i]] = (gates / (1.0 + jnp.exp(-gates)) * ups).astype(BF16)

    top = lax.broadcasted_iota(jnp.int32, (rows // 8, 8, wide), 1) < 4
    for i in range(split):
        low = dot_nn(hidden[...], down_ref[0, :, cols[i]]).reshape(-1, 8, wide)
        high = dot_nn(hidden[...], down_ref[0, :, half + i * wide : half + (i + 1) * wide]).reshape(-1, 8, wide)
        one = jnp.where(top, low, pltpu.roll(high, 4, 1))
        two = jnp.where(top, pltpu.roll(low, 4, 1), high)
        outs[i] = jnp.stack([one, two], axis=1).reshape(2 * rows, wide).astype(BF16)
        out_copies[i].start()
    for i in range(split):
        out_copies[i].wait()


def experts_on(slots, gate_matrix, up_matrix, down_matrix):
    rows, half = slots.shape
    width, inner = gate_matrix.shape[1:]
    split = 4
    here = pl.BlockSpec(memory_space=pltpu.VMEM)
    return pl.pallas_call(
        expert_kernel,
        in_specs=[here, here, here, here],
        out_specs=pl.BlockSpec(memory_space=pl.ANY),
        out_shape=pltpu.HBM((rows, half), BF16),
        scratch_shapes=[
            pltpu.VMEM((rows // 2, width), BF16),
            pltpu.VMEM((rows // 2, inner), BF16),
            pltpu.VMEM((split, rows, half // split), BF16),
            pltpu.SemaphoreType.DMA((split,)),
        ],
        compiler_params=params(24),
        name="experts_on",
    )(*map(in_vmem, (slots, gate_matrix, up_matrix, down_matrix)))


def combine_kernel(returned_ref, pick_ref, weight_ref, stream_ref, out_ref, stream_in, outs, sems):
    rows, _ = stream_in.shape
    half = returned_ref.shape[1]
    stream_copy = pltpu.make_async_copy(stream_ref, stream_in, sems.at[0])
    stream_copy.start()
    weights = weight_ref[...]
    wide = outs.shape[2]
    copies = []
    for n in range(half // wide):
        picked = dot_nn(pick_ref[...], returned_ref[:, n * wide : (n + 1) * wide])
        if n == 0:
            stream_copy.wait()
        for j in range(2):
            at = 2 * j * rows
            cols = slice(j * half + n * wide, j * half + (n + 1) * wide)
            added = weights[:, 0:1] * picked[at : at + rows] + weights[:, 1:2] * picked[at + rows : at + 2 * rows]
            slot = 2 * n + j
            outs[slot] = (stream_in[:, cols].astype(F32) + added).astype(BF16)
            copies.append(pltpu.make_async_copy(outs.at[slot], out_ref.at[:, cols], sems.at[slot + 1]))
            copies[-1].start()
    for copy in copies:
        copy.wait()


def combine(returned, pick, stream, routing_weight):
    rows, width = stream.shape
    here = pl.BlockSpec(memory_space=pltpu.VMEM)
    there = pl.BlockSpec(memory_space=pl.ANY)
    pieces = 4
    return pl.pallas_call(
        combine_kernel,
        in_specs=[here, here, here, there],
        out_specs=there,
        out_shape=pltpu.HBM(stream.shape, BF16),
        scratch_shapes=[
            pltpu.VMEM((rows, width), BF16),
            pltpu.VMEM((pieces, rows, width // pieces), BF16),
            pltpu.SemaphoreType.DMA((pieces + 1,)),
        ],
        compiler_params=params(24),
        name="combine",
    )(in_vmem(returned), in_vmem(pick), in_vmem(routing_weight), in_hbm(stream))


def body(
    resid,
    query,
    forget_logits,
    forget_margin,
    decay_spike,
    value_logits,
    output_gate_logits,
    head_norm_scale,
    output_matrix,
    norm_scale_vector,
    routes,
    routing_weight,
    gate_matrix,
    up_matrix,
    down_matrix,
):
    rows, top = routes.shape
    experts = lax.axis_size(SP) * lax.axis_size("tp")
    capacity = 2 * rows * top // experts
    width = resid.shape[1]
    margin = forget_margin[None, :]
    places = lax.axis_size("tp")
    cum, start, sent = local_states(forget_logits, value_logits, margin, decay_spike.T)
    select, pick = slots_of(routes, experts, capacity)
    parts = lax.all_to_all(sent, SP, split_axis=0, concat_axis=0, tiled=True)
    within, high, low, gates = within_blocks(
        query, forget_logits, margin, cum, value_logits, start, output_gate_logits, head_norm_scale[None, :]
    )
    prior = lax.all_to_all(carried_in(parts), SP, split_axis=0, concat_axis=0, tiled=True)
    prior = prior.reshape(start.shape[1], DK)
    shifts = (2, 1, places - 1)
    arrived = []
    for k in shifts:
        gated = gated_rows(k, within, high, low, prior, gates)
        arrived.append(lax.ppermute(gated, "tp", [(i, (i + k) % places) for i in range(places)]))
    total, matrix, select = project_own(within, high, low, prior, gates, output_matrix, resid, select)
    total = project_more(arrived[0], shifts[0], matrix, total)
    total = project_more(arrived[1], shifts[1], matrix, total)
    stream, packed = project(arrived[2], shifts[2], matrix, total, norm_scale_vector[None, :], select)
    shape = (experts, 2 * capacity, width // 2)
    slots = lax.all_to_all(packed.reshape(shape), SP_TP, split_axis=0, concat_axis=0, tiled=True)
    answers = experts_on(slots.reshape(packed.shape), gate_matrix, up_matrix, down_matrix)
    returned = lax.all_to_all(answers.reshape(shape), SP_TP, split_axis=0, concat_axis=0, tiled=True)
    return combine(returned.reshape(packed.shape), pick, stream, routing_weight)


def solution(mesh):
    finer = Mesh(mesh.devices.reshape(4, 4, 2, mesh.shape["tp"]), SP_TP)
    placed = (
        P(SP_TP, None),
        P(SP, "tp"),
        P(SP, "tp"),
        P("tp"),
        P(SP, "tp"),
        P(SP, "tp"),
        P(SP, "tp"),
        P("tp"),
        P(),
        P(),
        P(SP_TP, None),
        P(SP_TP, None),
        P(SP_TP, None, None),
        P(SP_TP, None, None),
        P(SP_TP, None, None),
    )
    return jax.shard_map(
        body, mesh=finer, in_specs=placed, out_specs=P(SP_TP, None), check_vma=False
    )
```
